256 devices in a mesh: sp: 16 (over y, x), dp: 16 (over z, core).
Axes of the slice: x: 4, y: 4, z: 8, core: 2. Of those that a mesh axis runs over, the one named last changes fastest.
Arguments:
- value_half: bfloat16 [16, 4096, 2048], P('dp', 'sp'), may hold values from -6 to 6
- gate_half: bfloat16 [16, 4096, 2048], P('dp', 'sp'), may hold values from -6 to 6
- upstream: bfloat16 [16, 4096, 2048], P('dp', 'sp'), may hold values from -6 to 6
- conv_taps: float32 [31, 2048], P(None, 'sp'), may hold values from -1 to 1
- norm_gain: float32 [2048], replicated, may hold values from 0.1 to 1.9
- out_weight: bfloat16 [2048, 2048], P('dp'), may hold values from -0.125 to 0.125
Outputs:
- grad_value: bfloat16 [16, 4096, 2048], P('dp', 'sp')
- grad_gate: bfloat16 [16, 4096, 2048], P('dp', 'sp')
- grad_taps: float32 [31, 2048], P(None, 'sp')
- grad_gain: float32 [2048], replicated
- grad_weight: float32 [2048, 2048], P('dp')
The draws below stay inside these ranges and needn't reach their ends.
All inputs are finite; a program needn't handle non-finite values.
Results may differ from the reference program's by a relative error of at most 0.0062.
Values may be sent and summed in bfloat16 or wider, within the bound.
No kernel may reach another device: no remote copies, remote signals or barrier semaphores. Data moves between devices by JAX's collectives and lax.ppermute only.
A program may use at most 128 MiB of HBM per device.

```python
import jax
import jax.numpy as jnp
from jax import lax

D = 2048
KERNEL = 31
LENGTH = 4096
BATCH = 16


def spiked(drawn, rng, source, target, parts, factor):
    owner, partner = [(jnp.arange(drawn.shape[dim]) // (drawn.shape[dim] // parts)).reshape([-1 if axis == dim else 1 for axis in range(drawn.ndim)]) for dim in (source, target)]
    chosen = jax.random.permutation(rng, parts)[partner]
    strong = (owner == chosen) | (owner == (partner + parts // 2) % parts)
    return jnp.where(strong, factor * drawn, drawn)


def block_levels(stream_key, dims, pieces, low, largest):
    level = 1.0
    for axis_at, blocks in pieces:
        draws = jax.random.uniform(jax.random.fold_in(jax.random.fold_in(stream_key, 6), axis_at), (blocks,), jnp.float32, low / len(pieces), largest / len(pieces))
        level = level * jnp.repeat(jnp.exp(draws), dims[axis_at] // blocks).reshape((-1,) + (1,) * (len(dims) - 1 - axis_at))
    return level


def normal_values(own_key, shape, scale, bound, pieces=(), held_as=jnp.bfloat16):
    drawn = scale * jax.random.normal(own_key, shape, jnp.float32)
    if pieces:
        drawn = drawn * block_levels(own_key, shape, pieces, -0.22, 0.18)
    return jnp.clip(drawn, -bound, bound).astype(held_as)


def bell_draw_with(rng, shape, spread, limit, cuts, heavy, dtype=jnp.bfloat16):
    drawn = spread * jax.random.normal(rng, shape, jnp.float32)
    if cuts:
        drawn = drawn * block_levels(rng, shape, cuts, -0.22, 0.18)
    return jnp.clip(spiked(drawn, jax.random.fold_in(rng, 3), *heavy), -limit, limit).astype(dtype)


def setup_inputs(seed: int = 0) -> dict:
    splits = jax.random.split(jax.random.key(seed), 7)
    return {
        "value_half": normal_values(splits[0], (BATCH, LENGTH, D), 1.0, 6.0, ((0, 16), (1, 16))),
        "gate_half": normal_values(splits[1], (BATCH, LENGTH, D), 1.0, 6.0, ((0, 16), (1, 16))),
        "upstream": bell_draw_with(splits[2], (BATCH, LENGTH, D), 1.0, 6.0, ((0, 16), (1, 16)), (0, 2, 16, 2.0)),
        "conv_taps": normal_values(splits[3], (KERNEL, D), 0.18, 1.0, ((1, 16),), jnp.float32),
        "norm_gain": jnp.clip(1.0 + 0.18 * jax.random.normal(splits[4], (D,), jnp.float32), 0.1, 1.9),
        "out_weight": normal_values(splits[5], (D, D), D ** -0.5, 0.125, ((0, 16),)),
    }


NORM_EPS = 1e-05

def one_sequence(sequence, conv_taps, norm_gain, out_weight):
    value_half, gate_half, upstream = sequence
    tap_count = conv_taps.shape[0]
    length = value_half.shape[0]
    sig_gate = jax.nn.sigmoid(gate_half.astype(jnp.float32))
    value_wide = value_half.astype(jnp.float32)
    glu = (value_wide * sig_gate).astype(jnp.bfloat16)
    glu_wide = lax.optimization_barrier(glu).astype(jnp.float32)
    padded = jnp.pad(glu_wide, ((tap_count - 1, 0), (0, 0)))
    conv_out = jnp.zeros_like(glu_wide)
    for offset in range(tap_count):
        conv_out = conv_out + conv_taps[offset] * padded[offset:offset + length]
    conv_out = lax.optimization_barrier(conv_out.astype(jnp.bfloat16)).astype(jnp.float32)
    row_mean = lax.optimization_barrier(jnp.mean(conv_out, axis=-1, keepdims=True))
    centered = conv_out - row_mean
    inv_scale = lax.rsqrt(lax.optimization_barrier(jnp.mean(centered * centered, axis=-1, keepdims=True)) + NORM_EPS)
    normed = centered * inv_scale
    scaled = normed * norm_gain
    sig_scaled = jax.nn.sigmoid(scaled)
    activated = (scaled * sig_scaled).astype(jnp.bfloat16)
    grad_act = jnp.dot(upstream, out_weight, preferred_element_type=jnp.float32)
    grad_scaled = grad_act * sig_scaled * (1.0 + scaled * (1.0 - sig_scaled))
    gain_term = lax.optimization_barrier(jnp.sum(grad_scaled * normed, axis=0))
    grad_normed = grad_scaled * norm_gain
    grad_conv_out = inv_scale * (grad_normed - lax.optimization_barrier(jnp.mean(grad_normed, axis=-1, keepdims=True)) - normed * lax.optimization_barrier(jnp.mean(grad_normed * normed, axis=-1, keepdims=True)))
    grad_conv_out = lax.optimization_barrier(grad_conv_out.astype(jnp.bfloat16)).astype(jnp.float32)
    grad_padded = jnp.pad(grad_conv_out, ((0, tap_count - 1), (0, 0)))
    grad_glu = jnp.zeros_like(grad_conv_out)
    tap_terms = []
    for offset in range(tap_count):
        first = tap_count - 1 - offset
        grad_glu = grad_glu + conv_taps[offset] * grad_padded[first:first + length]
        tap_terms.append(lax.optimization_barrier(jnp.sum(grad_conv_out * padded[offset:offset + length], axis=0)))
    grad_glu = lax.optimization_barrier(grad_glu.astype(jnp.bfloat16)).astype(jnp.float32)
    grad_value = (grad_glu * sig_gate).astype(jnp.bfloat16)
    grad_gate = (grad_glu * value_wide * sig_gate * (1.0 - sig_gate)).astype(jnp.bfloat16)
    return (grad_value, grad_gate, activated, jnp.stack(tap_terms), gain_term)

def reference(value_half, gate_half, upstream, conv_taps, norm_gain, out_weight):

    def mapped(sequence):
        return one_sequence(sequence, conv_taps, norm_gain, out_weight)
    grad_value, grad_gate, activated, tap_terms, gain_terms = lax.map(mapped, (value_half, gate_half, upstream))
    model_width = value_half.shape[2]
    grad_weight = lax.dot_general(upstream.reshape(-1, model_width), activated.reshape(-1, model_width), (((0,), (0,)), ((), ())), preferred_element_type=jnp.float32)
    grad_taps = lax.optimization_barrier(jnp.sum(tap_terms, axis=0))
    grad_gain = lax.optimization_barrier(jnp.sum(gain_terms, axis=0))
    return (grad_value, grad_gate, grad_taps, grad_gain, grad_weight)
```

```python
import functools

import jax
import jax.numpy as jnp
from jax import lax
from jax.experimental import pallas as pl
from jax.experimental.pallas import tpu as pltpu
from jax.sharding import Mesh
from jax.sharding import PartitionSpec as P

DP = ("dp_0", "dp_1")
SP = ("sp_0", "sp_1")
Y, X, Z, CORE = "sp_0", "sp_1", "dp_0", "dp_1"
NORM_EPS = 1e-05
HALO = 32
INTERPRET = False
F32, BF16 = jnp.float32, jnp.bfloat16


def call(kernel, grid, in_specs, out_specs, out_shape, scratch, flops=0, moved=0):
    return pl.pallas_call(
        kernel,
        grid_spec=pltpu.PrefetchScalarGridSpec(
            num_scalar_prefetch=1,
            grid=grid,
            in_specs=in_specs,
            out_specs=out_specs,
            scratch_shapes=scratch,
        ),
        out_shape=out_shape,
        compiler_params=pltpu.CompilerParams(
            dimension_semantics=("arbitrary",) * len(grid), vmem_limit_bytes=48 * 1024 * 1024
        ),
        cost_estimate=pl.CostEstimate(flops=flops, bytes_accessed=moved, transcendentals=0),
        interpret=INTERPRET,
    )


def shift(value, axis, amount):
    count = lax.axis_size(axis)
    return lax.ppermute(value, axis, [(i, (i + amount) % count) for i in range(count)])


def relative(ring, block):
    return lax.rem(block // 4 - ring[0] + 4, 4) * 4 + lax.rem(block % 4 - ring[1] + 4, 4)


def forward_kernel(ring, value, gate, halo, taps, gain, glu, act, conv, mean, inv, wide, held, total):
    block = pl.program_id(0)
    tokens, lanes = value.shape
    blocks = held.shape[0]
    gated = (value[...].astype(F32) * jax.nn.sigmoid(gate[...].astype(F32))).astype(BF16)
    glu[...] = gated
    wide[pl.ds(0, HALO), :] = halo[...].astype(F32)
    wide[pl.ds(HALO, tokens), :] = gated.astype(F32)
    acc = jnp.zeros((tokens, lanes), F32)
    for j in range(31):
        acc = acc + taps[0, pl.ds(j, 1), :] * wide[pl.ds(2 + j, tokens), :]
    rounded = acc.astype(BF16)
    conv[:, pl.ds(pl.multiple_of(block * lanes, lanes), lanes)] = rounded
    rounded = rounded.astype(F32)
    held[block] = rounded

    @pl.when(block == 0)
    def _():
        total[...] = rounded

    @pl.when(block > 0)
    def _():
        total[...] += rounded

    @pl.when(block == blocks - 1)
    def _():
        width = blocks * lanes
        mu = jnp.sum(total[...], axis=1, keepdims=True) / width
        mu = jnp.broadcast_to(mu, (tokens, lanes))
        mean[...] = mu

        def squares(i, acc):
            centered = held[i] - mean[...]
            return acc + centered * centered

        squared = lax.fori_loop(0, blocks, squares, jnp.zeros((tokens, lanes), F32))
        var = jnp.sum(squared, axis=1, keepdims=True) / width
        inv[...] = jnp.broadcast_to(lax.rsqrt(var + NORM_EPS), (tokens, lanes))

        def finish(i, carry):
            at = pl.ds(pl.multiple_of(i * lanes, lanes), lanes)
            scaled = (held[i] - mean[...]) * inv[...] * gain[:, at]
            act[:, at] = (scaled * jax.nn.sigmoid(scaled)).astype(BF16)
            return carry

        lax.fori_loop(0, blocks, finish, 0)


def forward(ring, value, gate, halo, taps, gain):
    tokens, width = value.shape
    lanes = width // 16
    column = lambda rows: pl.BlockSpec((rows, lanes), lambda i, ring: (0, i))
    whole = lambda *shape: pl.BlockSpec(shape, lambda i, ring: (0,) * len(shape))
    return call(
        forward_kernel,
        (16,),
        [
            column(tokens),
            column(tokens),
            column(HALO),
            pl.BlockSpec((1, 32, lanes), lambda i, ring: (relative(ring, i), 0, 0)),
            whole(1, width),
        ],
        [column(tokens), whole(tokens, width), whole(tokens, width), whole(tokens, lanes), whole(tokens, lanes)],
        [
            jax.ShapeDtypeStruct((tokens, width), BF16),
            jax.ShapeDtypeStruct((tokens, width), BF16),
            jax.ShapeDtypeStruct((tokens, width), BF16),
            jax.ShapeDtypeStruct((tokens, lanes), F32),
            jax.ShapeDtypeStruct((tokens, lanes), F32),
        ],
        [
            pltpu.VMEM((HALO + tokens, lanes), F32),
            pltpu.VMEM((16, tokens, lanes), F32),
            pltpu.VMEM((tokens, lanes), F32),
        ],
        flops=62 * tokens * width * 100,
        moved=10 * tokens * width,
    )(ring, value, gate, halo, taps, gain)


def turn_kernel(ring, upstream, own, other):
    lanes = own.shape[1]
    core = ring[3]
    mine = upstream[:, pl.ds(pl.multiple_of(core * lanes, lanes), lanes)].astype(F32)
    own[0] = mine.T.astype(BF16)
    theirs = upstream[:, pl.ds(pl.multiple_of((1 - core) * lanes, lanes), lanes)].astype(F32)
    other[0] = theirs.T.astype(BF16)


def turn(ring, upstream):
    tokens, width = upstream.shape
    lanes = width // 16
    out = pl.BlockSpec((1, lanes, tokens), lambda i, ring: (i, 0, 0))
    shape = jax.ShapeDtypeStruct((8, lanes, tokens), BF16)
    return call(
        turn_kernel,
        (8,),
        [pl.BlockSpec((tokens, 2 * lanes), lambda i, ring: (0, i))],
        [out, out],
        [shape, shape],
        [],
        flops=tokens * width * 100,
        moved=4 * tokens * width,
    )(ring, upstream)


def outer_kernel(plan, ring, turned, turned_other, act, act_other, *outs):
    lanes = turned.shape[1]
    tokens = turned.shape[2]
    y, x = ring[0], ring[1]

    def columns(source, ky, kx):
        block = lax.rem(y + ky, 4) * 4 + lax.rem(x + kx, 4)
        return source[:, pl.ds(pl.multiple_of(block * lanes, lanes), lanes)]

    for (half, k, pair), out in zip(plan, outs):
        rows = pl.ds(4 * half, 4)
        left = turned[rows].reshape(4 * lanes, tokens)
        left_other = turned_other[rows].reshape(4 * lanes, tokens)
        spots = [(2 * pair + i, k) if half == 0 else (k, 2 * pair + i) for i in range(2)]
        right = jnp.concatenate([columns(act, *spot) for spot in spots], axis=1)
        right_other = jnp.concatenate([columns(act_other, *spot) for spot in spots], axis=1)
        product = jnp.dot(left, right, preferred_element_type=F32)
        product = product + jnp.dot(left_other, right_other, preferred_element_type=F32)
        out[0] = product[:, :lanes].astype(BF16)
        out[1] = product[:, lanes:].astype(BF16)


def outer(plan, ring, turned, turned_other, act, act_other):
    tokens, width = act.shape
    lanes = width // 16
    whole = lambda *shape: pl.BlockSpec(shape, lambda i, ring: (0,) * len(shape))
    parts = call(
        functools.partial(outer_kernel, plan),
        (1,),
        [whole(8, lanes, tokens)] * 2 + [whole(tokens, width)] * 2,
        [whole(2, 4 * lanes, lanes)] * len(plan),
        [jax.ShapeDtypeStruct((2, 4 * lanes, lanes), BF16)] * len(plan),
        [],
        flops=2 * 2 * tokens * 8 * lanes * lanes * len(plan),
        moved=8 * tokens * width,
    )(ring, turned, turned_other, act, act_other)
    return dict(zip(plan, parts))


def add(*terms):
    return sum(term.astype(F32) for term in terms)


def tie(values, after):
    return lax.optimization_barrier((values, after))[0]


def ring_open(axis, piece):
    two_on = shift(piece(2, 0), axis, 1)
    two_back = shift(piece(2, 1), axis, -1)
    early_on = shift(piece(1, 1), axis, 1)
    early_back = shift(piece(3, 0), axis, -1)
    late_on = add(piece(1, 0), two_on).astype(BF16)
    late_back = add(piece(3, 1), two_back).astype(BF16)
    return early_on, early_back, late_on, late_back


def ring_close(axis, piece, early_on, early_back, late_on, late_back):
    late_on = shift(late_on, axis, 1)
    late_back = shift(late_back, axis, -1)
    return add(piece(0, 0), late_on, early_back), add(piece(0, 1), early_on, late_back)


def cut(low, high):
    held = {0: low[0], 1: low[1], 2: high[0], 3: high[1]}
    rows = held[0].shape[0] // 2
    held = {(k, h): held[k][h * rows : (h + 1) * rows] for k in held for h in range(2)}
    return {key: value.astype(BF16) if key[0] else value for key, value in held.items()}


def place_kernel(ring, blocks, out):
    out[...] = blocks[0].astype(F32)


def place(ring, blocks):
    count, rows, lanes = blocks.shape

    def spot(i, ring):
        return (0, lax.rem(ring[0] + i // 4, 4) * 4 + lax.rem(ring[1] + i % 4, 4))

    return call(
        place_kernel,
        (count,),
        [pl.BlockSpec((1, rows, lanes), lambda i, ring: (i, 0, 0))],
        pl.BlockSpec((rows, lanes), spot),
        jax.ShapeDtypeStruct((rows, count * lanes), F32),
        [],
        flops=count * rows * lanes,
        moved=6 * count * rows * lanes,
    )(ring, blocks)


def plane_row(shard):
    return jnp.stack([shard] + [shift(shard, X, -k) for k in range(1, 4)])


def plane_column(row):
    return jnp.concatenate([row] + [shift(row, Y, -k) for k in range(1, 4)])


def weight_step(got, k):
    if k < 4:
        for h in range(2):
            got[k, h] = shift(got[k - 1, h], Z, 1)
            got[8 - k, h] = shift(got[(9 - k) % 8, h], Z, -1)
    else:
        got[4, 0] = shift(got[3, 0], Z, 1)
        got[4, 1] = shift(got[5, 1], Z, -1)


def norm_kernel(ring, upstream, *refs):
    weights = refs[:32]
    conv, mean, inv, gain, grad, grad_head, gain_part, lhs, held, first, second = refs[32:]
    step = pl.program_id(0)
    steps = held.shape[0]
    _, lanes = mean.shape
    wide = 2 * lanes
    z, core = ring[2], ring[3]

    @pl.when(step == 0)
    def _():
        for k in range(8):
            chip = lax.rem(z - k + 8, 8) * wide
            for i, side in enumerate((core, 1 - core)):
                at = pl.multiple_of(chip + side * lanes, lanes)
                lhs[:, pl.ds((2 * k + i) * lanes, lanes)] = upstream[:, pl.ds(at, lanes)]
        first[...] = jnp.zeros_like(first)
        second[...] = jnp.zeros_like(second)

    rhs = jnp.concatenate([weight[...] for weight in weights], axis=0)
    grad_act = jnp.dot(lhs[...], rhs, preferred_element_type=F32)
    for i in range(2):
        at = slice(i * lanes, (i + 1) * lanes)
        columns = pl.ds(pl.multiple_of((2 * step + i) * lanes, lanes), lanes)
        normed = (conv[:, columns].astype(F32) - mean[...]) * inv[...]
        scaled = normed * gain[:, at]
        sig = jax.nn.sigmoid(scaled)
        grad_scaled = grad_act[:, at] * sig * (1.0 + scaled * (1.0 - sig))
        gain_part[:, at] = jnp.sum(grad_scaled * normed, axis=0, keepdims=True)
        g = grad_scaled * gain[:, at]
        held[step, :, at] = g
        first[...] += g
        second[...] += g * normed

    @pl.when(step == steps - 1)
    def _():
        width = steps * wide
        first[...] = jnp.broadcast_to(jnp.sum(first[...], axis=1, keepdims=True) / width, first.shape)
        second[...] = jnp.broadcast_to(jnp.sum(second[...], axis=1, keepdims=True) / width, second.shape)

        def finish(i, carry):
            for j in range(2):
                at = slice(j * lanes, (j + 1) * lanes)
                to = pl.ds(pl.multiple_of((2 * i + j) * lanes, lanes), lanes)
                normed = (conv[:, to].astype(F32) - mean[...]) * inv[...]
                value = (inv[...] * (held[i, :, at] - first[...] - normed * second[...])).astype(BF16)
                grad[:, to] = value
                grad_head[:, to] = value[:HALO]
            return carry

        lax.fori_loop(0, steps, finish, 0)


def norm_backward(ring, upstream, weights, conv, mean, inv, gain):
    tokens, width = upstream.shape
    lanes = width // 16
    wide = 2 * lanes
    column = lambda rows: pl.BlockSpec((rows, wide), lambda i, ring: (0, i))
    whole = lambda *shape: pl.BlockSpec(shape, lambda i, ring: (0,) * len(shape))
    return call(
        norm_kernel,
        (8,),
        [whole(tokens, width)]
        + [column(weight.shape[0]) for weight in weights]
        + [whole(tokens, width), whole(tokens, lanes), whole(tokens, lanes), column(1)],
        [whole(tokens, width), whole(HALO, width), column(1)],
        [
            jax.ShapeDtypeStruct((tokens, width), BF16),
            jax.ShapeDtypeStruct((HALO, width), BF16),
            jax.ShapeDtypeStruct((1, width), F32),
        ],
        [
            pltpu.VMEM((tokens, width), BF16),
            pltpu.VMEM((8, tokens, wide), F32),
            pltpu.VMEM((tokens, lanes), F32),
            pltpu.VMEM((tokens, lanes), F32),
        ],
        flops=2 * tokens * width * width,
        moved=2 * width * width + 6 * tokens * width,
    )(ring, upstream, *weights, conv, mean, inv, gain)


def taps_kernel(ring, glu, halo, grad, gain_part, out, wide):
    tokens, _ = glu.shape
    wide[pl.ds(0, HALO), :] = halo[...].astype(F32)
    wide[pl.ds(HALO, tokens), :] = glu[...].astype(F32)
    g = grad[...].astype(F32)
    for j in range(31):
        out[0, pl.ds(j, 1), :] = jnp.sum(g * wide[pl.ds(2 + j, tokens), :], axis=0, keepdims=True)
    out[0, pl.ds(31, 1), :] = gain_part[...]


def taps_backward(ring, glu, halo, grad, gain_part):
    tokens, width = glu.shape
    lanes = width // 16
    column = lambda rows: pl.BlockSpec((rows, lanes), lambda i, ring: (0, i))
    return call(
        taps_kernel,
        (16,),
        [column(tokens), column(HALO), column(tokens), column(1)],
        pl.BlockSpec((1, 32, lanes), lambda i, ring: (i, 0, 0)),
        jax.ShapeDtypeStruct((16, 32, lanes), F32),
        [pltpu.VMEM((HALO + tokens, lanes), F32)],
        flops=62 * tokens * width * 100,
        moved=4 * tokens * width,
    )(ring, glu, halo, grad, gain_part)


def input_kernel(ring, grad, tail, taps, value, gate, grad_value, grad_gate, wide):
    tokens, lanes = grad.shape
    wide[pl.ds(0, tokens), :] = grad[...].astype(F32)
    wide[pl.ds(tokens, HALO), :] = tail[...].astype(F32)
    acc = jnp.zeros((tokens, lanes), F32)
    for j in range(31):
        acc = acc + taps[0, pl.ds(j, 1), :] * wide[pl.ds(30 - j, tokens), :]
    grad_glu = acc.astype(BF16).astype(F32)
    sig = jax.nn.sigmoid(gate[...].astype(F32))
    grad_value[...] = (grad_glu * sig).astype(BF16)
    grad_gate[...] = (grad_glu * value[...].astype(F32) * sig * (1.0 - sig)).astype(BF16)


def input_backward(ring, grad, tail, taps, value, gate):
    tokens, width = grad.shape
    lanes = width // 16
    column = lambda rows: pl.BlockSpec((rows, lanes), lambda i, ring: (0, i))
    return call(
        input_kernel,
        (16,),
        [
            column(tokens),
            column(HALO),
            pl.BlockSpec((1, 32, lanes), lambda i, ring: (relative(ring, i), 0, 0)),
            column(tokens),
            column(tokens),
        ],
        [column(tokens)] * 2,
        [jax.ShapeDtypeStruct((tokens, width), BF16)] * 2,
        [pltpu.VMEM((HALO + tokens, lanes), F32)],
        flops=62 * tokens * width * 100,
        moved=10 * tokens * width,
    )(ring, grad, tail, taps, value, gate)


def from_everyone(shard, axis):
    count = lax.axis_size(axis)
    return lax.all_to_all(jnp.broadcast_to(shard[None], (count, *shard.shape)), axis, 0, 0, tiled=True)


PLAN = [(half, k, pair) for k in (2, 1, 3, 0) for pair in range(2) for half in range(2)]


def step(value_half, gate_half, upstream, conv_taps, norm_gain, out_weight):
    value, gate, upstream = value_half[0], gate_half[0], upstream[0]
    tokens, width = value.shape
    lanes = width // 16
    ring = jnp.stack([lax.axis_index(axis) for axis in (Y, X, Z, CORE)]).astype(jnp.int32)
    gain = norm_gain[None]

    tail = slice(tokens - HALO, tokens)
    glu_tail = (value[tail].astype(F32) * jax.nn.sigmoid(gate[tail].astype(F32))).astype(BF16)
    halo = lax.ppermute(glu_tail, SP, [(i, i + 1) for i in range(15)])
    taps = plane_column(plane_row(jnp.pad(conv_taps, ((0, 1), (0, 0)))))

    rows = out_weight.shape[0] // 2
    side = {(0, h): out_weight[h * rows : (h + 1) * rows] for h in range(2)}
    weight_step(side, 1)

    turned, turned_away = turn(ring, upstream)
    turned_other = shift(turned_away, CORE, 1)
    value_in, turned = lax.optimization_barrier((value, turned))

    glu, act, conv, mean, inv = forward(ring, value_in, gate, halo, taps, gain)
    act_other = shift(act, CORE, 1)

    def hold(step, after):
        for k in (step, 8 - step):
            for h in range(2):
                side[k, h] = tie(side[k, h], after)

    hold(1, act)
    weight_step(side, 2)

    parts = outer(PLAN, ring, turned, turned_other, act, act_other)
    hold(2, parts[PLAN[0]])
    weight_step(side, 3)

    pieces = [lambda k, h, half=half: parts[half, k, h] for half in range(2)]
    opened = [ring_open(axis, piece) for axis, piece in zip((X, Y), pieces)]
    hold(3, [part for half in opened for part in half[2:]])
    weight_step(side, 4)
    pieces = [cut(*ring_close(axis, piece, *half)) for axis, piece, half in zip((X, Y), pieces, opened)]
    pieces = [lambda k, h, held=held: held[k, h] for held in pieces]
    opened = [ring_open(axis, piece) for axis, piece in zip((Y, X), pieces)]
    closed = [ring_close(axis, piece, *half) for axis, piece, half in zip((Y, X), pieces, opened)]
    scattered = jnp.concatenate([rows for half in closed for rows in half]).astype(BF16).reshape(8, lanes, lanes)

    across = {key: shift(piece, CORE, 1) for key, piece in side.items()}
    weights = [source[k, h] for k in range(8) for source in (side, across) for h in range(2)]
    owned = lax.all_to_all(scattered, Z, 0, 0, tiled=True)
    grad, grad_head, gain_part = norm_backward(ring, tie(upstream, scattered), weights, conv, mean, inv, gain)
    next_head = lax.ppermute(grad_head, SP, [(i + 1, i) for i in range(15)])
    owned = jnp.sum(tie(owned, grad).astype(F32), axis=0).astype(BF16)

    terms = taps_backward(ring, glu, halo, tie(grad, owned), gain_part)
    row = plane_row(owned)
    mine = lax.all_to_all(terms, SP, 0, 0, tiled=True)
    grad_value, grad_gate = input_backward(ring, tie(grad, row), next_head, taps, value, gate)
    mine = jnp.sum(tie(mine, grad_value), axis=0)
    grad_weight = place(ring, tie(plane_column(row), grad_value))
    mine = jnp.sum(from_everyone(mine, DP), axis=0)
    grad_taps = mine[:31]
    grad_gain = from_everyone(mine[31:], SP).reshape(width)
    return grad_value[None], grad_gate[None], grad_taps, grad_gain, grad_weight


def solution(mesh):
    torus = Mesh(mesh.devices.reshape(4, 4, 8, 2), (Y, X, Z, CORE))
    placed = (P(DP, SP, None), P(DP, SP, None), P(DP, SP, None), P(None, SP), P(), P(DP, None))
    return jax.shard_map(
        step,
        mesh=torus,
        in_specs=placed,
        out_specs=(P(DP, SP, None), P(DP, SP, None), P(None, SP), P(), P(DP, None)),
        check_vma=False,
    )
```

```python
import functools

import jax
import jax.numpy as jnp
from jax import lax
from jax.experimental import pallas as pl
from jax.experimental.pallas import tpu as pltpu
from jax.sharding import Mesh
from jax.sharding import PartitionSpec as P

DP = ("dp_0", "dp_1")
SP = ("sp_0", "sp_1")
Y, X, Z, CORE = "sp_0", "sp_1", "dp_0", "dp_1"
NORM_EPS = 1e-05
HALO = 32
INTERPRET = False
F32, BF16 = jnp.float32, jnp.bfloat16


def call(kernel, name, grid, in_specs, out_specs, out_shape, scratch, flops=0, moved=0):
    return pl.pallas_call(
        kernel,
        name=name,
        grid_spec=pltpu.PrefetchScalarGridSpec(
            num_scalar_prefetch=1,
            grid=grid,
            in_specs=in_specs,
            out_specs=out_specs,
            scratch_shapes=scratch,
        ),
        out_shape=out_shape,
        compiler_params=pltpu.CompilerParams(
            dimension_semantics=("arbitrary",) * len(grid), vmem_limit_bytes=48 * 1024 * 1024
        ),
        cost_estimate=pl.CostEstimate(flops=flops, bytes_accessed=moved, transcendentals=0),
        interpret=INTERPRET,
    )


def shift(value, axis, amount):
    count = lax.axis_size(axis)
    return lax.ppermute(value, axis, [(i, (i + amount) % count) for i in range(count)])


def relative(ring, block):
    return lax.rem(block // 4 - ring[0] + 4, 4) * 4 + lax.rem(block % 4 - ring[1] + 4, 4)


def forward_kernel(ring, value, gate, halo, taps, gain, glu, act, conv, mean, inv, wide, held, total):
    block = pl.program_id(0)
    tokens, lanes = value.shape
    blocks = held.shape[0]
    gated = (value[...].astype(F32) * jax.nn.sigmoid(gate[...].astype(F32))).astype(BF16)
    glu[...] = gated
    wide[pl.ds(0, HALO), :] = halo[...].astype(F32)
    wide[pl.ds(HALO, tokens), :] = gated.astype(F32)
    acc = jnp.zeros((tokens, lanes), F32)
    for j in range(31):
        acc = acc + taps[0, pl.ds(j, 1), :] * wide[pl.ds(2 + j, tokens), :]
    rounded = acc.astype(BF16)
    conv[:, pl.ds(pl.multiple_of(block * lanes, lanes), lanes)] = rounded
    rounded = rounded.astype(F32)
    held[block] = rounded

    @pl.when(block == 0)
    def _():
        total[...] = rounded

    @pl.when(block > 0)
    def _():
        total[...] += rounded

    @pl.when(block == blocks - 1)
    def _():
        width = blocks * lanes
        mu = jnp.sum(total[...], axis=1, keepdims=True) / width
        mu = jnp.broadcast_to(mu, (tokens, lanes))
        mean[...] = mu

        def squares(i, acc):
            centered = held[i] - mean[...]
            return acc + centered * centered

        squared = lax.fori_loop(0, blocks, squares, jnp.zeros((tokens, lanes), F32))
        var = jnp.sum(squared, axis=1, keepdims=True) / width
        inv[...] = jnp.broadcast_to(lax.rsqrt(var + NORM_EPS), (tokens, lanes))

        def finish(i, carry):
            at = pl.ds(pl.multiple_of(i * lanes, lanes), lanes)
            scaled = (held[i] - mean[...]) * inv[...] * gain[:, at]
            act[:, at] = (scaled * jax.nn.sigmoid(scaled)).astype(BF16)
            return carry

        lax.fori_loop(0, blocks, finish, 0)


def forward(ring, value, gate, halo, taps, gain):
    tokens, width = value.shape
    lanes = width // 16
    column = lambda rows: pl.BlockSpec((rows, lanes), lambda i, ring: (0, i))
    whole = lambda *shape: pl.BlockSpec(shape, lambda i, ring: (0,) * len(shape))
    return call(
        forward_kernel,
        "forward",
        (16,),
        [
            column(tokens),
            column(tokens),
            column(HALO),
            pl.BlockSpec((1, 32, lanes), lambda i, ring: (relative(ring, i), 0, 0)),
            whole(1, width),
        ],
        [column(tokens), whole(tokens, width), whole(tokens, width), whole(tokens, lanes), whole(tokens, lanes)],
        [
            jax.ShapeDtypeStruct((tokens, width), BF16),
            jax.ShapeDtypeStruct((tokens, width), BF16),
            jax.ShapeDtypeStruct((tokens, width), BF16),
            jax.ShapeDtypeStruct((tokens, lanes), F32),
            jax.ShapeDtypeStruct((tokens, lanes), F32),
        ],
        [
            pltpu.VMEM((HALO + tokens, lanes), F32),
            pltpu.VMEM((16, tokens, lanes), F32),
            pltpu.VMEM((tokens, lanes), F32),
        ],
        flops=62 * tokens * width * 100,
        moved=10 * tokens * width,
    )(ring, value, gate, halo, taps, gain)


def turn_kernel(ring, upstream, own, other):
    lanes = own.shape[1]
    core = ring[3]
    mine = upstream[:, pl.ds(pl.multiple_of(core * lanes, lanes), lanes)].astype(F32)
    own[0] = mine.T.astype(BF16)
    theirs = upstream[:, pl.ds(pl.multiple_of((1 - core) * lanes, lanes), lanes)].astype(F32)
    other[0] = theirs.T.astype(BF16)


def turn(ring, upstream):
    tokens, width = upstream.shape
    lanes = width // 16
    out = pl.BlockSpec((1, lanes, tokens), lambda i, ring: (i, 0, 0))
    shape = jax.ShapeDtypeStruct((8, lanes, tokens), BF16)
    return call(
        turn_kernel,
        "turn",
        (8,),
        [pl.BlockSpec((tokens, 2 * lanes), lambda i, ring: (0, i))],
        [out, out],
        [shape, shape],
        [],
        flops=tokens * width * 100,
        moved=4 * tokens * width,
    )(ring, upstream)


def outer_kernel(plan, ring, turned, turned_other, act, act_other, *outs):
    lanes = turned.shape[1]
    tokens = turned.shape[2]
    y, x = ring[0], ring[1]

    def columns(source, ky, kx):
        block = lax.rem(y + ky, 4) * 4 + lax.rem(x + kx, 4)
        return source[:, pl.ds(pl.multiple_of(block * lanes, lanes), lanes)]

    for half, k, pair, target, at in plan:
        out = outs[target]
        rows = pl.ds(4 * half, 4)
        left = turned[rows].reshape(4 * lanes, tokens)
        left_other = turned_other[rows].reshape(4 * lanes, tokens)
        spots = [(2 * pair + i, k) if half == 0 else (k, 2 * pair + i) for i in range(2)]
        right = jnp.concatenate([columns(act, *spot) for spot in spots], axis=1)
        right_other = jnp.concatenate([columns(act_other, *spot) for spot in spots], axis=1)
        product = jnp.dot(left, right, preferred_element_type=F32)
        product = product + jnp.dot(left_other, right_other, preferred_element_type=F32)
        out[at] = product[:, :lanes].astype(BF16)
        out[at + 1] = product[:, lanes:].astype(BF16)


def outer(plan, ring, turned, turned_other, act, act_other):
    tokens, width = act.shape
    lanes = width // 16
    whole = lambda *shape: pl.BlockSpec(shape, lambda i, ring: (0,) * len(shape))
    sizes = [max(at for *_, target, at in plan if target == out) + 2 for out in range(plan[-1][3] + 1)]
    return call(
        functools.partial(outer_kernel, plan),
        "outer",
        (1,),
        [whole(8, lanes, tokens)] * 2 + [whole(tokens, width)] * 2,
        [whole(size, 4 * lanes, lanes) for size in sizes],
        [jax.ShapeDtypeStruct((size, 4 * lanes, lanes), BF16) for size in sizes],
        [],
        flops=2 * 2 * tokens * 8 * lanes * lanes * len(plan),
        moved=8 * tokens * width,
    )(ring, turned, turned_other, act, act_other)


def add(*terms):
    return sum(term.astype(F32) for term in terms)


def tie(values, after):
    return lax.optimization_barrier((values, after))[0]


def ring_open(axis, on, back):
    return shift(on, axis, 1), shift(back, axis, -1)


def ring_sums(opened, next_low, previous_high):
    on, back = opened
    count = on.shape[0] // 2
    return add(next_low, on[:count]).astype(BF16), add(previous_high, back[:count]).astype(BF16)


def ring_close(axis, opened, sums, own_low, own_high):
    on, back = opened
    count = on.shape[0] // 2
    late_on = shift(sums[0], axis, 1)
    late_back = shift(sums[1], axis, -1)
    return add(own_low, late_on, back[count:]), add(own_high, on[count:], late_back)


def cut(low, high):
    rows = low.shape[1] // 2
    block = lambda k, h: (low, high)[k // 2][k % 2, h * rows : (h + 1) * rows]
    on = jnp.concatenate([block(2, 0), block(1, 1)]).astype(BF16)
    back = jnp.concatenate([block(2, 1), block(3, 0)]).astype(BF16)
    return (on, back), (block(1, 0), block(3, 1)), (block(0, 0), block(0, 1))


def place_kernel(ring, blocks, out):
    count, _, lanes = blocks.shape
    for i in range(count):
        block = lax.rem(ring[0] + i // 4, 4) * 4 + lax.rem(ring[1] + i % 4, 4)
        out[:, pl.ds(pl.multiple_of(block * lanes, lanes), lanes)] = blocks[i].astype(F32)


def place(ring, blocks):
    count, rows, lanes = blocks.shape
    whole = lambda *shape: pl.BlockSpec(shape, lambda i, ring: (0,) * len(shape))
    return call(
        place_kernel,
        "place",
        (1,),
        [whole(count, rows, lanes)],
        whole(rows, count * lanes),
        jax.ShapeDtypeStruct((rows, count * lanes), F32),
        [],
        flops=count * rows * lanes,
        moved=6 * count * rows * lanes,
    )(ring, blocks)


def plane_row(shard):
    return jnp.stack([shard] + [shift(shard, X, -k) for k in range(1, 4)])


def plane_column(row):
    return jnp.concatenate([row] + [shift(row, Y, -k) for k in range(1, 4)])


def norm_kernel(
    ring, upstream, weight, conv, mean, inv, gain, grad, grad_head, gain_part, held, first, second
):
    step = pl.program_id(0)
    steps = held.shape[0]
    tokens, lanes = mean.shape
    wide = 2 * lanes

    @pl.when(step == 0)
    def _():
        first[...] = jnp.zeros_like(first)
        second[...] = jnp.zeros_like(second)

    grad_act = jnp.dot(upstream[...], weight[...], preferred_element_type=F32)
    for i in range(2):
        at = slice(i * lanes, (i + 1) * lanes)
        columns = pl.ds(pl.multiple_of((2 * step + i) * lanes, lanes), lanes)
        normed = (conv[:, columns].astype(F32) - mean[...]) * inv[...]
        scaled = normed * gain[:, at]
        sig = jax.nn.sigmoid(scaled)
        grad_scaled = grad_act[:, at] * sig * (1.0 + scaled * (1.0 - sig))
        gain_part[:, at] = jnp.sum(grad_scaled * normed, axis=0, keepdims=True)
        g = grad_scaled * gain[:, at]
        held[step, :, at] = g
        first[...] += g
        second[...] += g * normed

    @pl.when(step == steps - 1)
    def _():
        width = steps * wide
        first[...] = jnp.broadcast_to(jnp.sum(first[...], axis=1, keepdims=True) / width, first.shape)
        second[...] = jnp.broadcast_to(jnp.sum(second[...], axis=1, keepdims=True) / width, second.shape)

        def finish(i, carry):
            for j in range(2):
                at = slice(j * lanes, (j + 1) * lanes)
                to = pl.ds(pl.multiple_of((2 * i + j) * lanes, lanes), lanes)
                normed = (conv[:, to].astype(F32) - mean[...]) * inv[...]
                value = (inv[...] * (held[i, :, at] - first[...] - normed * second[...])).astype(BF16)
                grad[:, to] = value
                grad_head[:, to] = value[:HALO]
            return carry

        lax.fori_loop(0, steps, finish, 0)


def norm_backward(ring, upstream, weight, conv, mean, inv, gain):
    tokens, width = upstream.shape
    lanes = width // 16
    wide = 2 * lanes
    column = lambda rows: pl.BlockSpec((rows, wide), lambda i, ring: (0, i))
    whole = lambda *shape: pl.BlockSpec(shape, lambda i, ring: (0,) * len(shape))
    return call(
        norm_kernel,
        "norm_backward",
        (8,),
        [
            whole(tokens, width),
            column(width),
            whole(tokens, width),
            whole(tokens, lanes),
            whole(tokens, lanes),
            column(1),
        ],
        [whole(tokens, width), whole(HALO, width), column(1)],
        [
            jax.ShapeDtypeStruct((tokens, width), BF16),
            jax.ShapeDtypeStruct((HALO, width), BF16),
            jax.ShapeDtypeStruct((1, width), F32),
        ],
        [
            pltpu.VMEM((8, tokens, wide), F32),
            pltpu.VMEM((tokens, lanes), F32),
            pltpu.VMEM((tokens, lanes), F32),
        ],
        flops=2 * tokens * width * width,
        moved=2 * width * width + 6 * tokens * width,
    )(ring, upstream, weight, conv, mean, inv, gain)


def taps_kernel(ring, glu, halo, grad, gain_part, out, wide):
    tokens, lanes = glu.shape
    wide[pl.ds(0, HALO), :] = halo[...].astype(F32)
    wide[pl.ds(HALO, tokens), :] = glu[...].astype(F32)
    g = grad[...].astype(F32)
    for j in range(31):
        out[0, pl.ds(j, 1), :] = jnp.sum(g * wide[pl.ds(2 + j, tokens), :], axis=0, keepdims=True)
    out[0, pl.ds(31, 1), :] = gain_part[...]


def taps_backward(ring, glu, halo, grad, gain_part):
    tokens, width = glu.shape
    lanes = width // 16
    column = lambda rows: pl.BlockSpec((rows, lanes), lambda i, ring: (0, i))
    return call(
        taps_kernel,
        "taps_backward",
        (16,),
        [column(tokens), column(HALO), column(tokens), column(1)],
        pl.BlockSpec((1, 32, lanes), lambda i, ring: (i, 0, 0)),
        jax.ShapeDtypeStruct((16, 32, lanes), F32),
        [pltpu.VMEM((HALO + tokens, lanes), F32)],
        flops=62 * tokens * width * 100,
        moved=4 * tokens * width,
    )(ring, glu, halo, grad, gain_part)


def input_kernel(ring, grad, tail, taps, value, gate, grad_value, grad_gate, wide):
    tokens, lanes = grad.shape
    wide[pl.ds(0, tokens), :] = grad[...].astype(F32)
    wide[pl.ds(tokens, HALO), :] = tail[...].astype(F32)
    acc = jnp.zeros((tokens, lanes), F32)
    for j in range(31):
        acc = acc + taps[0, pl.ds(j, 1), :] * wide[pl.ds(30 - j, tokens), :]
    grad_glu = acc.astype(BF16).astype(F32)
    sig = jax.nn.sigmoid(gate[...].astype(F32))
    grad_value[...] = (grad_glu * sig).astype(BF16)
    grad_gate[...] = (grad_glu * value[...].astype(F32) * sig * (1.0 - sig)).astype(BF16)


def input_backward(ring, grad, tail, taps, value, gate):
    tokens, width = grad.shape
    lanes = width // 16
    column = lambda rows: pl.BlockSpec((rows, lanes), lambda i, ring: (0, i))
    return call(
        input_kernel,
        "input_backward",
        (16,),
        [
            column(tokens),
            column(HALO),
            pl.BlockSpec((1, 32, lanes), lambda i, ring: (relative(ring, i), 0, 0)),
            column(tokens),
            column(tokens),
        ],
        [column(tokens)] * 2,
        [jax.ShapeDtypeStruct((tokens, width), BF16)] * 2,
        [pltpu.VMEM((HALO + tokens, lanes), F32)],
        flops=62 * tokens * width * 100,
        moved=10 * tokens * width,
    )(ring, grad, tail, taps, value, gate)


def from_everyone(shard, axis):
    count = lax.axis_size(axis)
    return lax.all_to_all(jnp.broadcast_to(shard[None], (count, *shard.shape)), axis, 0, 0, tiled=True)


PLAN = [
    (half, k, pair, 5 * half + out, at)
    for half in range(2)
    for k, pair, out, at in (
        (2, 0, 0, 0),
        (1, 1, 0, 2),
        (2, 1, 1, 0),
        (3, 0, 1, 2),
        (1, 0, 2, 0),
        (3, 1, 3, 0),
        (0, 0, 4, 0),
        (0, 1, 4, 2),
    )
]


def body(value_half, gate_half, upstream, conv_taps, norm_gain, out_weight):
    value, gate, upstream = value_half[0], gate_half[0], upstream[0]
    tokens, width = value.shape
    lanes = width // 16
    ring = jnp.stack([lax.axis_index(axis) for axis in (Y, X, Z, CORE)]).astype(jnp.int32)
    gain = norm_gain[None]

    tail = slice(tokens - HALO, tokens)
    glu_tail = (value[tail].astype(F32) * jax.nn.sigmoid(gate[tail].astype(F32))).astype(BF16)
    halo = lax.ppermute(glu_tail, SP, [(i, i + 1) for i in range(15)])
    taps = plane_column(plane_row(jnp.pad(conv_taps, ((0, 1), (0, 0)))))

    weight = lax.all_gather(out_weight, DP, axis=0, tiled=True)

    turned, turned_away = turn(ring, upstream)
    turned_other = shift(turned_away, CORE, 1)
    value_in, turned = lax.optimization_barrier((value, turned))

    glu, act, conv, mean, inv = forward(ring, value_in, gate, halo, taps, gain)
    act_other = shift(act, CORE, 1)
    parts = outer(PLAN, ring, turned, turned_other, act, act_other)
    parts = [parts[:5], parts[5:]]

    opened = [ring_open(axis, *part[:2]) for axis, part in zip((X, Y), parts)]
    sums = [ring_sums(pair, *part[2:4]) for pair, part in zip(opened, parts)]
    halves = [
        ring_close(axis, pair, late, part[4][:2], part[4][2:])
        for axis, pair, late, part in zip((X, Y), opened, sums, parts)
    ]
    grad, grad_head, gain_part = norm_backward(ring, tie(upstream, sums), weight, conv, mean, inv, gain)
    next_head = lax.ppermute(grad_head, SP, [(i + 1, i) for i in range(15)])

    pieces = [cut(*half) for half in tie(halves, grad)]
    opened = [ring_open(axis, *piece[0]) for axis, piece in zip((Y, X), pieces)]
    terms = taps_backward(ring, glu, halo, tie(grad, [piece[0] for piece in pieces]), gain_part)
    opened = tie(opened, terms)
    sums = [ring_sums(pair, *piece[1]) for pair, piece in zip(opened, pieces)]
    mine = lax.all_to_all(tie(terms, sums), SP, 0, 0, tiled=True)
    closed = [
        ring_close(axis, pair, late, *piece[2]) for axis, pair, late, piece in zip((Y, X), opened, sums, pieces)
    ]
    scattered = jnp.concatenate([rows for half in closed for rows in half]).astype(BF16).reshape(8, lanes, lanes)
    owned = lax.all_to_all(scattered, Z, 0, 0, tiled=True)

    grad_value, grad_gate = input_backward(ring, tie(grad, scattered), next_head, taps, value, gate)
    mine = jnp.sum(tie(mine, grad_value), axis=0)
    mine = from_everyone(mine, DP)
    owned = jnp.sum(tie(owned, grad_value).astype(F32), axis=0).astype(BF16)
    blocks = plane_column(plane_row(owned))
    mine = jnp.sum(mine, axis=0)
    grad_taps = mine[:31]
    grad_gain = from_everyone(mine[31:], SP).reshape(width)
    grad_weight = place(ring, blocks)
    return grad_value[None], grad_gate[None], grad_taps, grad_gain, grad_weight


def solution(mesh):
    torus = Mesh(mesh.devices.reshape(4, 4, 8, 2), (Y, X, Z, CORE))
    placed = (P(DP, SP, None), P(DP, SP, None), P(DP, SP, None), P(None, SP), P(), P(DP, None))
    return jax.shard_map(
        body,
        mesh=torus,
        in_specs=placed,
        out_specs=(P(DP, SP, None), P(DP, SP, None), P(None, SP), P(), P(DP, None)),
        check_vma=False,
    )
```

```python
import functools

import jax
import jax.numpy as jnp
from jax import lax
from jax.experimental import pallas as pl
from jax.experimental.pallas import tpu as pltpu
from jax.sharding import Mesh
from jax.sharding import PartitionSpec as P

DP = ("dp_0", "dp_1")
SP = ("sp_0", "sp_1")
Y, X, Z, CORE = "sp_0", "sp_1", "dp_0", "dp_1"
NORM_EPS = 1e-05
HALO = 32
GROUP = 4
INTERPRET = False
F32, BF16 = jnp.float32, jnp.bfloat16


def call(kernel, grid, in_specs, out_specs, out_shape, scratch, flops=0, moved=0):
    return pl.pallas_call(
        kernel,
        grid_spec=pltpu.PrefetchScalarGridSpec(
            num_scalar_prefetch=1,
            grid=grid,
            in_specs=in_specs,
            out_specs=out_specs,
            scratch_shapes=scratch,
        ),
        out_shape=out_shape,
        compiler_params=pltpu.CompilerParams(
            dimension_semantics=("arbitrary",) * len(grid), vmem_limit_bytes=48 * 1024 * 1024
        ),
        cost_estimate=pl.CostEstimate(flops=flops, bytes_accessed=moved, transcendentals=0),
        interpret=INTERPRET,
    )


def shift(value, axis, amount):
    count = lax.axis_size(axis)
    return lax.ppermute(value, axis, [(i, (i + amount) % count) for i in range(count)])


def forward_kernel(ring, value, gate, halo, taps, gain, glu, act, conv, mean, inv, wide, held, total):
    step = pl.program_id(0)
    tokens = value.shape[0]
    blocks, _, lanes = held.shape

    @pl.when(step == 0)
    def _():
        total[...] = jnp.zeros_like(total)

    for i in range(GROUP):
        at = slice(i * lanes, (i + 1) * lanes)
        block = step * GROUP + i
        gated = (value[:, at].astype(F32) * jax.nn.sigmoid(gate[:, at].astype(F32))).astype(BF16)
        glu[:, at] = gated
        wide[i, pl.ds(0, HALO), :] = halo[:, at].astype(F32)
        wide[i, pl.ds(HALO, tokens), :] = gated.astype(F32)
        acc = jnp.zeros((tokens, lanes), F32)
        for j in range(31):
            acc = acc + taps[i, pl.ds(j, 1), :] * wide[i, pl.ds(2 + j, tokens), :]
        rounded = acc.astype(BF16)
        conv[:, pl.ds(pl.multiple_of(block * lanes, lanes), lanes)] = rounded
        rounded = rounded.astype(F32)
        held[block] = rounded
        total[...] += rounded

    @pl.when(step == pl.num_programs(0) - 1)
    def _():
        width = blocks * lanes
        mu = jnp.sum(total[...], axis=1, keepdims=True) / width
        mu = jnp.broadcast_to(mu, (tokens, lanes))
        mean[...] = mu

        def squares(i, acc):
            centered = held[i] - mean[...]
            return acc + centered * centered

        squared = lax.fori_loop(0, blocks, squares, jnp.zeros((tokens, lanes), F32))
        var = jnp.sum(squared, axis=1, keepdims=True) / width
        inv[...] = jnp.broadcast_to(lax.rsqrt(var + NORM_EPS), (tokens, lanes))

        def finish(i, carry):
            at = pl.ds(pl.multiple_of(i * lanes, lanes), lanes)
            scaled = (held[i] - mean[...]) * inv[...] * gain[:, at]
            act[:, at] = (scaled * jax.nn.sigmoid(scaled)).astype(BF16)
            return carry

        lax.fori_loop(0, blocks, finish, 0)


def forward(ring, value, gate, halo, taps, gain):
    tokens, width = value.shape
    lanes = width // 16
    column = lambda rows: pl.BlockSpec((rows, GROUP * lanes), lambda i, ring: (0, i))
    whole = lambda *shape: pl.BlockSpec(shape, lambda i, ring: (0,) * len(shape))
    return call(
        forward_kernel,
        (16 // GROUP,),
        [
            column(tokens),
            column(tokens),
            column(HALO),
            pl.BlockSpec((GROUP, 32, lanes), lambda i, ring: (i, 0, 0)),
            whole(1, width),
        ],
        [column(tokens), whole(tokens, width), whole(tokens, width), whole(tokens, lanes), whole(tokens, lanes)],
        [
            jax.ShapeDtypeStruct((tokens, width), BF16),
            jax.ShapeDtypeStruct((tokens, width), BF16),
            jax.ShapeDtypeStruct((tokens, width), BF16),
            jax.ShapeDtypeStruct((tokens, lanes), F32),
            jax.ShapeDtypeStruct((tokens, lanes), F32),
        ],
        [
            pltpu.VMEM((GROUP, HALO + tokens, lanes), F32),
            pltpu.VMEM((16, tokens, lanes), F32),
            pltpu.VMEM((tokens, lanes), F32),
        ],
        flops=62 * tokens * width * 100,
        moved=10 * tokens * width,
    )(ring, value, gate, halo, taps, gain)


def turn_kernel(ring, upstream, own, other):
    lanes = own.shape[1]
    core = ring[3]
    mine = upstream[:, pl.ds(pl.multiple_of(core * lanes, lanes), lanes)].astype(F32)
    own[0] = mine.T.astype(BF16)
    theirs = upstream[:, pl.ds(pl.multiple_of((1 - core) * lanes, lanes), lanes)].astype(F32)
    other[0] = theirs.T.astype(BF16)


def turn(ring, upstream):
    tokens, width = upstream.shape
    lanes = width // 16
    out = pl.BlockSpec((1, lanes, tokens), lambda i, ring: (i, 0, 0))
    shape = jax.ShapeDtypeStruct((8, lanes, tokens), BF16)
    return call(
        turn_kernel,
        (8,),
        [pl.BlockSpec((tokens, 2 * lanes), lambda i, ring: (0, i))],
        [out, out],
        [shape, shape],
        [],
        flops=tokens * width * 100,
        moved=4 * tokens * width,
    )(ring, upstream)


def outer_kernel(plan, ring, turned, turned_other, act, act_other, *outs):
    lanes = turned.shape[1]
    tokens = turned.shape[2]
    y, x = ring[0], ring[1]

    def columns(source, ky, kx):
        block = lax.rem(y + ky, 4) * 4 + lax.rem(x + kx, 4)
        return source[:, pl.ds(pl.multiple_of(block * lanes, lanes), lanes)]

    for half, k, pair, target, at in plan:
        out = outs[target]
        rows = pl.ds(4 * half, 4)
        left = turned[rows].reshape(4 * lanes, tokens)
        left_other = turned_other[rows].reshape(4 * lanes, tokens)
        spots = [(2 * pair + i, k) if half == 0 else (k, 2 * pair + i) for i in range(2)]
        right = jnp.concatenate([columns(act, *spot) for spot in spots], axis=1)
        right_other = jnp.concatenate([columns(act_other, *spot) for spot in spots], axis=1)
        product = jnp.dot(left, right, preferred_element_type=F32)
        product = product + jnp.dot(left_other, right_other, preferred_element_type=F32)
        out[at] = product[:, :lanes].astype(BF16)
        out[at + 1] = product[:, lanes:].astype(BF16)


def outer(plan, ring, turned, turned_other, act, act_other):
    tokens, width = act.shape
    lanes = width // 16
    whole = lambda *shape: pl.BlockSpec(shape, lambda i, ring: (0,) * len(shape))
    sizes = [max(at for *_, target, at in plan if target == out) + 2 for out in range(plan[-1][3] + 1)]
    return call(
        functools.partial(outer_kernel, plan),
        (1,),
        [whole(8, lanes, tokens)] * 2 + [whole(tokens, width)] * 2,
        [whole(size, 4 * lanes, lanes) for size in sizes],
        [jax.ShapeDtypeStruct((size, 4 * lanes, lanes), BF16) for size in sizes],
        [],
        flops=2 * 2 * tokens * 8 * lanes * lanes * len(plan),
        moved=8 * tokens * width,
    )(ring, turned, turned_other, act, act_other)


def add(*terms):
    return sum(term.astype(F32) for term in terms)


def tie(values, after):
    return lax.optimization_barrier((values, after))[0]


def ring_open(axis, on, back):
    return shift(on, axis, 1), shift(back, axis, -1)


def ring_sums(opened, next_low, previous_high):
    on, back = opened
    count = on.shape[0] // 2
    return add(next_low, on[:count]).astype(BF16), add(previous_high, back[:count]).astype(BF16)


def ring_close(axis, opened, sums, own_low, own_high):
    on, back = opened
    count = on.shape[0] // 2
    late_on = shift(sums[0], axis, 1)
    late_back = shift(sums[1], axis, -1)
    return add(own_low, late_on, back[count:]), add(own_high, on[count:], late_back)


def cut(low, high):
    rows = low.shape[1] // 2
    block = lambda k, h: (low, high)[k // 2][k % 2, h * rows : (h + 1) * rows]
    on = jnp.concatenate([block(2, 0), block(1, 1)]).astype(BF16)
    back = jnp.concatenate([block(2, 1), block(3, 0)]).astype(BF16)
    return (on, back), (block(1, 0), block(3, 1)), (block(0, 0), block(0, 1))


def place_kernel(ring, blocks, out):
    count, _, lanes = blocks.shape
    for i in range(count):
        block = lax.rem(ring[0] + i // 4, 4) * 4 + lax.rem(ring[1] + i % 4, 4)
        out[:, pl.ds(pl.multiple_of(block * lanes, lanes), lanes)] = blocks[i].astype(F32)


def place(ring, blocks):
    count, rows, lanes = blocks.shape
    whole = lambda *shape: pl.BlockSpec(shape, lambda i, ring: (0,) * len(shape))
    return call(
        place_kernel,
        (1,),
        [whole(count, rows, lanes)],
        whole(rows, count * lanes),
        jax.ShapeDtypeStruct((rows, count * lanes), F32),
        [],
        flops=count * rows * lanes,
        moved=6 * count * rows * lanes,
    )(ring, blocks)


def plane_row(shard):
    return jnp.stack([shard] + [shift(shard, X, -k) for k in range(1, 4)])


def plane_column(row):
    return jnp.concatenate([row] + [shift(row, Y, -k) for k in range(1, 4)])


def norm_kernel(
    ring, upstream, weight, conv, mean, inv, gain, grad, grad_head, gain_part, held, first, second
):
    step = pl.program_id(0)
    steps = held.shape[0]
    _, lanes = mean.shape
    wide = 2 * lanes

    @pl.when(step == 0)
    def _():
        first[...] = jnp.zeros_like(first)
        second[...] = jnp.zeros_like(second)

    grad_act = jnp.dot(upstream[...], weight[...], preferred_element_type=F32)
    for i in range(2):
        at = slice(i * lanes, (i + 1) * lanes)
        columns = pl.ds(pl.multiple_of((2 * step + i) * lanes, lanes), lanes)
        normed = (conv[:, columns].astype(F32) - mean[...]) * inv[...]
        scaled = normed * gain[:, at]
        sig = jax.nn.sigmoid(scaled)
        grad_scaled = grad_act[:, at] * sig * (1.0 + scaled * (1.0 - sig))
        gain_part[pl.ds(2 * step + i, 1), :] = jnp.sum(grad_scaled * normed, axis=0, keepdims=True)
        g = grad_scaled * gain[:, at]
        held[step, :, at] = g
        first[...] += g
        second[...] += g * normed

    @pl.when(step == steps - 1)
    def _():
        width = steps * wide
        first[...] = jnp.broadcast_to(jnp.sum(first[...], axis=1, keepdims=True) / width, first.shape)
        second[...] = jnp.broadcast_to(jnp.sum(second[...], axis=1, keepdims=True) / width, second.shape)

        def finish(i, carry):
            for j in range(2):
                at = slice(j * lanes, (j + 1) * lanes)
                to = pl.ds(pl.multiple_of((2 * i + j) * lanes, lanes), lanes)
                normed = (conv[:, to].astype(F32) - mean[...]) * inv[...]
                value = (inv[...] * (held[i, :, at] - first[...] - normed * second[...])).astype(BF16)
                grad[:, to] = value
                grad_head[:, to] = value[:HALO]
            return carry

        lax.fori_loop(0, steps, finish, 0)


def norm_backward(ring, upstream, weight, conv, mean, inv, gain):
    tokens, width = upstream.shape
    lanes = width // 16
    wide = 2 * lanes
    column = lambda rows: pl.BlockSpec((rows, wide), lambda i, ring: (0, i))
    whole = lambda *shape: pl.BlockSpec(shape, lambda i, ring: (0,) * len(shape))
    return call(
        norm_kernel,
        (8,),
        [
            whole(tokens, width),
            column(width),
            whole(tokens, width),
            whole(tokens, lanes),
            whole(tokens, lanes),
            column(1),
        ],
        [whole(tokens, width), whole(HALO, width), whole(16, lanes)],
        [
            jax.ShapeDtypeStruct((tokens, width), BF16),
            jax.ShapeDtypeStruct((HALO, width), BF16),
            jax.ShapeDtypeStruct((16, lanes), F32),
        ],
        [
            pltpu.VMEM((8, tokens, wide), F32),
            pltpu.VMEM((tokens, lanes), F32),
            pltpu.VMEM((tokens, lanes), F32),
        ],
        flops=2 * tokens * width * width,
        moved=2 * width * width + 6 * tokens * width,
    )(ring, upstream, weight, conv, mean, inv, gain)


def taps_kernel(ring, glu, halo, grad, gain_part, out, wide):
    tokens = glu.shape[0]
    lanes = wide.shape[2]
    for i in range(GROUP):
        at = slice(i * lanes, (i + 1) * lanes)
        wide[i, pl.ds(0, HALO), :] = halo[:, at].astype(F32)
        wide[i, pl.ds(HALO, tokens), :] = glu[:, at].astype(F32)
        g = grad[:, at].astype(F32)
        for j in range(31):
            out[i, pl.ds(j, 1), :] = jnp.sum(g * wide[i, pl.ds(2 + j, tokens), :], axis=0, keepdims=True)
        out[i, pl.ds(31, 1), :] = jnp.zeros((1, lanes), F32)
        out[i, pl.ds(32, 16), :] = gain_part[...]


def taps_backward(ring, glu, halo, grad, gain_part):
    tokens, width = glu.shape
    lanes = width // 16
    column = lambda rows: pl.BlockSpec((rows, GROUP * lanes), lambda i, ring: (0, i))
    return call(
        taps_kernel,
        (16 // GROUP,),
        [column(tokens), column(HALO), column(tokens), pl.BlockSpec((16, lanes), lambda i, ring: (0, 0))],
        pl.BlockSpec((GROUP, 48, lanes), lambda i, ring: (i, 0, 0)),
        jax.ShapeDtypeStruct((16, 48, lanes), F32),
        [pltpu.VMEM((GROUP, HALO + tokens, lanes), F32)],
        flops=62 * tokens * width * 100,
        moved=4 * tokens * width,
    )(ring, glu, halo, grad, gain_part)


def input_kernel(ring, grad, tail, taps, value, gate, grad_value, grad_gate, wide):
    tokens = grad.shape[0]
    lanes = wide.shape[2]
    for i in range(GROUP):
        at = slice(i * lanes, (i + 1) * lanes)
        wide[i, pl.ds(0, tokens), :] = grad[:, at].astype(F32)
        wide[i, pl.ds(tokens, HALO), :] = tail[:, at].astype(F32)
        acc = jnp.zeros((tokens, lanes), F32)
        for j in range(31):
            acc = acc + taps[i, pl.ds(j, 1), :] * wide[i, pl.ds(30 - j, tokens), :]
        grad_glu = acc.astype(BF16).astype(F32)
        sig = jax.nn.sigmoid(gate[:, at].astype(F32))
        grad_value[:, at] = (grad_glu * sig).astype(BF16)
        grad_gate[:, at] = (grad_glu * value[:, at].astype(F32) * sig * (1.0 - sig)).astype(BF16)


def input_backward(ring, grad, tail, taps, value, gate):
    tokens, width = grad.shape
    lanes = width // 16
    column = lambda rows: pl.BlockSpec((rows, GROUP * lanes), lambda i, ring: (0, i))
    return call(
        input_kernel,
        (16 // GROUP,),
        [
            column(tokens),
            column(HALO),
            pl.BlockSpec((GROUP, 32, lanes), lambda i, ring: (i, 0, 0)),
            column(tokens),
            column(tokens),
        ],
        [column(tokens)] * 2,
        [jax.ShapeDtypeStruct((tokens, width), BF16)] * 2,
        [pltpu.VMEM((GROUP, HALO + tokens, lanes), F32)],
        flops=62 * tokens * width * 100,
        moved=10 * tokens * width,
    )(ring, grad, tail, taps, value, gate)


def from_everyone(shard, axis):
    count = lax.axis_size(axis)
    return lax.all_to_all(jnp.broadcast_to(shard[None], (count, *shard.shape)), axis, 0, 0, tiled=True)


EARLY = [
    (half, k, pair, 2 * half + out, at)
    for half in range(2)
    for k, pair, out, at in ((2, 0, 0, 0), (1, 1, 0, 2), (2, 1, 1, 0), (3, 0, 1, 2))
]
REST = [
    (half, k, pair, 3 * half + out, at)
    for half in range(2)
    for k, pair, out, at in ((1, 0, 0, 0), (3, 1, 1, 0), (0, 0, 2, 0), (0, 1, 2, 2))
]


def step(value_half, gate_half, upstream, conv_taps, norm_gain, out_weight):
    value, gate, upstream = value_half[0], gate_half[0], upstream[0]
    tokens, width = value.shape
    lanes = width // 16
    ring = jnp.stack([lax.axis_index(axis) for axis in (Y, X, Z, CORE)]).astype(jnp.int32)
    gain = norm_gain[None]

    weight = lax.all_gather(out_weight, DP, axis=0, tiled=True)
    tail = slice(tokens - HALO, tokens)
    glu_tail = (value[tail].astype(F32) * jax.nn.sigmoid(gate[tail].astype(F32))).astype(BF16)
    halo = lax.ppermute(glu_tail, SP, [(i, i + 1) for i in range(15)])
    taps = from_everyone(jnp.pad(conv_taps, ((0, 1), (0, 0))), SP)

    turned, turned_away = turn(ring, upstream)
    turned_other = shift(turned_away, CORE, 1)

    glu, act, conv, mean, inv = forward(ring, value, gate, halo, taps, tie(gain, turned))
    act_other = shift(act, CORE, 1)
    early = outer(EARLY, ring, turned, turned_other, act, act_other)
    rest = outer(REST, ring, turned, turned_other, act, act_other)
    early, rest = (early[:2], early[2:]), (rest[:3], rest[3:])

    opened = [ring_open(axis, *part) for axis, part in zip((X, Y), early)]
    sums = [ring_sums(pair, *part[:2]) for pair, part in zip(opened, rest)]
    halves = [
        ring_close(axis, pair, late, part[2][:2], part[2][2:])
        for axis, pair, late, part in zip((X, Y), opened, sums, rest)
    ]
    grad, grad_head, gain_part = norm_backward(ring, upstream, weight, conv, mean, inv, tie(gain, sums))
    next_head = lax.ppermute(grad_head, SP, [(i + 1, i) for i in range(15)])

    pieces = [cut(*half) for half in halves]
    opened = [ring_open(axis, *piece[0]) for axis, piece in zip((Y, X), pieces)]
    sums = [ring_sums(pair, *piece[1]) for pair, piece in zip(opened, pieces)]
    closed = [ring_close(axis, pair, late, *piece[2]) for axis, pair, late, piece in zip((Y, X), opened, sums, pieces)]
    terms = taps_backward(ring, glu, halo, grad, gain_part)
    mine = lax.all_to_all(terms, SP, 0, 0, tiled=True)
    mine = jnp.sum(mine, axis=0)
    mine = mine + shift(mine, CORE, 1)

    scattered = jnp.concatenate([rows for half in closed for rows in half]).reshape(8, lanes, lanes)
    merged = jnp.concatenate([scattered, jnp.broadcast_to(mine[None], (8, *mine.shape))], axis=1)
    merged = lax.all_to_all(merged, Z, 0, 0, tiled=True)
    merged = jnp.sum(merged, axis=0)
    grad_value, grad_gate = input_backward(ring, grad, next_head, taps, value, gate)

    owned, mine = merged[:lanes].astype(BF16), merged[lanes:]
    grad_weight = place(ring, plane_column(plane_row(owned)))
    grad_taps = mine[:31]
    grad_gain = mine[32:].reshape(width)
    return grad_value[None], grad_gate[None], grad_taps, grad_gain, grad_weight


def solution(mesh):
    torus = Mesh(mesh.devices.reshape(4, 4, 8, 2), (Y, X, Z, CORE))
    placed = (P(DP, SP, None), P(DP, SP, None), P(DP, SP, None), P(None, SP), P(), P(DP, None))
    return jax.shard_map(
        step,
        mesh=torus,
        in_specs=placed,
        out_specs=(P(DP, SP, None), P(DP, SP, None), P(None, SP), P(), P(DP, None)),
        check_vma=False,
    )
```

```python
import functools

import jax
import jax.numpy as jnp
from jax import lax
from jax.experimental import pallas as pl
from jax.experimental.pallas import tpu as pltpu
from jax.sharding import Mesh
from jax.sharding import PartitionSpec as P

DP = ("dp_0", "dp_1")
SP = ("sp_0", "sp_1")
Y, X, Z, CORE = "sp_0", "sp_1", "dp_0", "dp_1"
NORM_EPS = 1e-05
HALO = 32
GROUP = 4
VMEM_LIMIT = 60
INTERPRET = False
F32, BF16 = jnp.float32, jnp.bfloat16


def call(kernel, grid, in_specs, out_specs, out_shape, scratch, flops=0, moved=0):
    return pl.pallas_call(
        kernel,
        grid_spec=pltpu.PrefetchScalarGridSpec(
            num_scalar_prefetch=1,
            grid=grid,
            in_specs=in_specs,
            out_specs=out_specs,
            scratch_shapes=scratch,
        ),
        out_shape=out_shape,
        compiler_params=pltpu.CompilerParams(
            dimension_semantics=("arbitrary",) * len(grid), vmem_limit_bytes=VMEM_LIMIT * 1024 * 1024
        ),
        cost_estimate=pl.CostEstimate(flops=flops, bytes_accessed=moved, transcendentals=0),
        interpret=INTERPRET,
    )


def shift(value, axis, amount):
    count = lax.axis_size(axis)
    return lax.ppermute(value, axis, [(i, (i + amount) % count) for i in range(count)])


def forward_kernel(ring, value, gate, halo, taps, gain, glu, act, conv, mean, inv, wide, held, total):
    step = pl.program_id(0)
    start = ring[0] + ring[1] == 0
    tokens = value.shape[0]
    blocks, _, lanes = held.shape

    @pl.when(step == 0)
    def _():
        total[...] = jnp.zeros_like(total)

    for i in range(GROUP):
        at = slice(i * lanes, (i + 1) * lanes)
        block = step * GROUP + i
        gated = (value[:, at].astype(F32) * jax.nn.sigmoid(gate[:, at].astype(F32))).astype(BF16)
        glu[:, at] = gated
        wide[i, pl.ds(0, HALO), :] = jnp.where(start, 0.0, halo[:, at].astype(F32))
        wide[i, pl.ds(HALO, tokens), :] = gated.astype(F32)
        acc = jnp.zeros((tokens, lanes), F32)
        for j in range(31):
            acc = acc + taps[i, pl.ds(j, 1), :] * wide[i, pl.ds(2 + j, tokens), :]
        rounded = acc.astype(BF16)
        conv[:, pl.ds(pl.multiple_of(block * lanes, lanes), lanes)] = rounded
        rounded = rounded.astype(F32)
        held[block] = rounded
        total[...] += rounded

    @pl.when(step == pl.num_programs(0) - 1)
    def _():
        width = blocks * lanes
        mu = jnp.sum(total[...], axis=1, keepdims=True) / width
        mu = jnp.broadcast_to(mu, (tokens, lanes))
        mean[...] = mu

        def squares(i, acc):
            centered = held[i] - mean[...]
            return acc + centered * centered

        squared = lax.fori_loop(0, blocks, squares, jnp.zeros((tokens, lanes), F32))
        var = jnp.sum(squared, axis=1, keepdims=True) / width
        inv[...] = jnp.broadcast_to(lax.rsqrt(var + NORM_EPS), (tokens, lanes))

        def finish(i, carry):
            at = pl.ds(pl.multiple_of(i * lanes, lanes), lanes)
            scaled = (held[i] - mean[...]) * inv[...] * gain[:, at]
            act[:, at] = (scaled * jax.nn.sigmoid(scaled)).astype(BF16)
            return carry

        lax.fori_loop(0, blocks, finish, 0)


def forward(ring, value, gate, halo, taps, gain):
    tokens, width = value.shape
    lanes = width // 16
    column = lambda rows: pl.BlockSpec((rows, GROUP * lanes), lambda i, ring: (0, i))
    whole = lambda *shape: pl.BlockSpec(shape, lambda i, ring: (0,) * len(shape))
    return call(
        forward_kernel,
        (16 // GROUP,),
        [
            column(tokens),
            column(tokens),
            column(HALO),
            pl.BlockSpec((GROUP, 32, lanes), lambda i, ring: (i, 0, 0)),
            whole(1, width),
        ],
        [column(tokens), whole(tokens, width), whole(tokens, width), whole(tokens, lanes), whole(tokens, lanes)],
        [
            jax.ShapeDtypeStruct((tokens, width), BF16),
            jax.ShapeDtypeStruct((tokens, width), BF16),
            jax.ShapeDtypeStruct((tokens, width), BF16),
            jax.ShapeDtypeStruct((tokens, lanes), F32),
            jax.ShapeDtypeStruct((tokens, lanes), F32),
        ],
        [
            pltpu.VMEM((GROUP, HALO + tokens, lanes), F32),
            pltpu.VMEM((16, tokens, lanes), F32),
            pltpu.VMEM((tokens, lanes), F32),
        ],
        flops=62 * tokens * width * 100,
        moved=10 * tokens * width,
    )(ring, value, gate, halo, taps, gain)


def turn_kernel(ring, upstream, own, other):
    lanes = own.shape[1]
    core = ring[3]
    mine = upstream[:, pl.ds(pl.multiple_of(core * lanes, lanes), lanes)].astype(F32)
    own[0] = mine.T.astype(BF16)
    theirs = upstream[:, pl.ds(pl.multiple_of((1 - core) * lanes, lanes), lanes)].astype(F32)
    other[0] = theirs.T.astype(BF16)


def turn(ring, upstream):
    tokens, width = upstream.shape
    lanes = width // 16
    out = pl.BlockSpec((1, lanes, tokens), lambda i, ring: (i, 0, 0))
    shape = jax.ShapeDtypeStruct((8, lanes, tokens), BF16)
    return call(
        turn_kernel,
        (8,),
        [pl.BlockSpec((tokens, 2 * lanes), lambda i, ring: (0, i))],
        [out, out],
        [shape, shape],
        [],
        flops=tokens * width * 100,
        moved=4 * tokens * width,
    )(ring, upstream)


def outer_kernel(plan, ring, turned, turned_other, act, act_other, *outs):
    lanes = turned.shape[1]
    tokens = turned.shape[2]
    y, x = ring[0], ring[1]

    def columns(source, ky, kx):
        block = lax.rem(y + ky, 4) * 4 + lax.rem(x + kx, 4)
        return source[:, pl.ds(pl.multiple_of(block * lanes, lanes), lanes)]

    for half, k, pair, target, at in plan:
        out = outs[target]
        rows = pl.ds(4 * half, 4)
        left = turned[rows].reshape(4 * lanes, tokens)
        left_other = turned_other[rows].reshape(4 * lanes, tokens)
        spots = [(2 * pair + i, k) if half == 0 else (k, 2 * pair + i) for i in range(2)]
        right = jnp.concatenate([columns(act, *spot) for spot in spots], axis=1)
        right_other = jnp.concatenate([columns(act_other, *spot) for spot in spots], axis=1)
        product = jnp.dot(left, right, preferred_element_type=F32)
        product = product + jnp.dot(left_other, right_other, preferred_element_type=F32)
        out[at] = product[:, :lanes].astype(BF16)
        out[at + 1] = product[:, lanes:].astype(BF16)


def outer(plan, ring, turned, turned_other, act, act_other):
    tokens, width = act.shape
    lanes = width // 16
    whole = lambda *shape: pl.BlockSpec(shape, lambda i, ring: (0,) * len(shape))
    sizes = [max(at for *_, target, at in plan if target == out) + 2 for out in range(plan[-1][3] + 1)]
    return call(
        functools.partial(outer_kernel, plan),
        (1,),
        [whole(8, lanes, tokens)] * 2 + [whole(tokens, width)] * 2,
        [whole(size, 4 * lanes, lanes) for size in sizes],
        [jax.ShapeDtypeStruct((size, 4 * lanes, lanes), BF16) for size in sizes],
        [],
        flops=2 * 2 * tokens * 8 * lanes * lanes * len(plan),
        moved=8 * tokens * width,
    )(ring, turned, turned_other, act, act_other)


def add(*terms):
    return sum(term.astype(F32) for term in terms)


def tie(values, after):
    return lax.optimization_barrier((values, after))[0]


def ring_open(axis, on, back):
    return shift(on, axis, 1), shift(back, axis, -1)


def ring_sums(opened, next_low, previous_high):
    on, back = opened
    count = on.shape[0] // 2
    return add(next_low, on[:count]).astype(BF16), add(previous_high, back[:count]).astype(BF16)


def ring_close(axis, opened, sums, own_low, own_high):
    on, back = opened
    count = on.shape[0] // 2
    late_on = shift(sums[0], axis, 1)
    late_back = shift(sums[1], axis, -1)
    return add(own_low, late_on, back[count:]), add(own_high, on[count:], late_back)


def cut(low, high):
    rows = low.shape[1] // 2
    block = lambda k, h: (low, high)[k // 2][k % 2, h * rows : (h + 1) * rows]
    on = jnp.concatenate([block(2, 0), block(1, 1)]).astype(BF16)
    back = jnp.concatenate([block(2, 1), block(3, 0)]).astype(BF16)
    return (on, back), (block(1, 0), block(3, 1)), (block(0, 0), block(0, 1))


def place_kernel(ring, blocks, out):
    count, _, lanes = blocks.shape
    for i in range(count):
        block = lax.rem(ring[0] + i // 4, 4) * 4 + lax.rem(ring[1] + i % 4, 4)
        out[:, pl.ds(pl.multiple_of(block * lanes, lanes), lanes)] = blocks[i].astype(F32)


def place(ring, blocks):
    count, rows, lanes = blocks.shape
    whole = lambda *shape: pl.BlockSpec(shape, lambda i, ring: (0,) * len(shape))
    return call(
        place_kernel,
        (1,),
        [whole(count, rows, lanes)],
        whole(rows, count * lanes),
        jax.ShapeDtypeStruct((rows, count * lanes), F32),
        [],
        flops=count * rows * lanes,
        moved=6 * count * rows * lanes,
    )(ring, blocks)


def plane_row(shard):
    return jnp.stack([shard] + [shift(shard, X, -k) for k in range(1, 4)])


def plane_column(row):
    return jnp.concatenate([row] + [shift(row, Y, -k) for k in range(1, 4)])


def norm_kernel(
    ring, upstream, weight, conv, mean, inv, gain, grad, grad_head, gain_part, held, first, second
):
    step = pl.program_id(0)
    steps = held.shape[0]
    _, lanes = mean.shape
    wide = 2 * lanes

    @pl.when(step == 0)
    def _():
        first[...] = jnp.zeros_like(first)
        second[...] = jnp.zeros_like(second)

    grad_act = jnp.dot(upstream[...], weight[...], preferred_element_type=F32)
    for i in range(2):
        at = slice(i * lanes, (i + 1) * lanes)
        columns = pl.ds(pl.multiple_of((2 * step + i) * lanes, lanes), lanes)
        normed = (conv[:, columns].astype(F32) - mean[...]) * inv[...]
        scaled = normed * gain[:, at]
        sig = jax.nn.sigmoid(scaled)
        grad_scaled = grad_act[:, at] * sig * (1.0 + scaled * (1.0 - sig))
        gain_part[pl.ds(2 * step + i, 1), :] = jnp.sum(grad_scaled * normed, axis=0, keepdims=True)
        g = grad_scaled * gain[:, at]
        held[step, :, at] = g
        first[...] += g
        second[...] += g * normed

    @pl.when(step == steps - 1)
    def _():
        width = steps * wide
        first[...] = jnp.broadcast_to(jnp.sum(first[...], axis=1, keepdims=True) / width, first.shape)
        second[...] = jnp.broadcast_to(jnp.sum(second[...], axis=1, keepdims=True) / width, second.shape)

        def finish(i, carry):
            for j in range(2):
                at = slice(j * lanes, (j + 1) * lanes)
                to = pl.ds(pl.multiple_of((2 * i + j) * lanes, lanes), lanes)
                normed = (conv[:, to].astype(F32) - mean[...]) * inv[...]
                value = (inv[...] * (held[i, :, at] - first[...] - normed * second[...])).astype(BF16)
                grad[:, to] = value
                grad_head[:, to] = value[:HALO]
            return carry

        lax.fori_loop(0, steps, finish, 0)


def norm_backward(ring, upstream, weight, conv, mean, inv, gain):
    tokens, width = upstream.shape
    lanes = width // 16
    wide = 2 * lanes
    column = lambda rows: pl.BlockSpec((rows, wide), lambda i, ring: (0, i))
    whole = lambda *shape: pl.BlockSpec(shape, lambda i, ring: (0,) * len(shape))
    return call(
        norm_kernel,
        (8,),
        [
            whole(tokens, width),
            column(width),
            whole(tokens, width),
            whole(tokens, lanes),
            whole(tokens, lanes),
            column(1),
        ],
        [whole(tokens, width), whole(HALO, width), whole(16, lanes)],
        [
            jax.ShapeDtypeStruct((tokens, width), BF16),
            jax.ShapeDtypeStruct((HALO, width), BF16),
            jax.ShapeDtypeStruct((16, lanes), F32),
        ],
        [
            pltpu.VMEM((8, tokens, wide), F32),
            pltpu.VMEM((tokens, lanes), F32),
            pltpu.VMEM((tokens, lanes), F32),
        ],
        flops=2 * tokens * width * width,
        moved=2 * width * width + 6 * tokens * width,
    )(ring, upstream, weight, conv, mean, inv, gain)


def taps_kernel(ring, glu, halo, grad, gain_part, out, wide):
    start = ring[0] + ring[1] == 0
    tokens = glu.shape[0]
    lanes = wide.shape[2]
    for i in range(GROUP):
        at = slice(i * lanes, (i + 1) * lanes)
        wide[i, pl.ds(0, HALO), :] = jnp.where(start, 0.0, halo[:, at].astype(F32))
        wide[i, pl.ds(HALO, tokens), :] = glu[:, at].astype(F32)
        g = grad[:, at].astype(F32)
        for j in range(31):
            out[i, pl.ds(j, 1), :] = jnp.sum(g * wide[i, pl.ds(2 + j, tokens), :], axis=0, keepdims=True)
        out[i, pl.ds(31, 1), :] = jnp.zeros((1, lanes), F32)
        out[i, pl.ds(32, 16), :] = gain_part[...]


def taps_backward(ring, glu, halo, grad, gain_part):
    tokens, width = glu.shape
    lanes = width // 16
    column = lambda rows: pl.BlockSpec((rows, GROUP * lanes), lambda i, ring: (0, i))
    return call(
        taps_kernel,
        (16 // GROUP,),
        [column(tokens), column(HALO), column(tokens), pl.BlockSpec((16, lanes), lambda i, ring: (0, 0))],
        pl.BlockSpec((GROUP, 48, lanes), lambda i, ring: (i, 0, 0)),
        jax.ShapeDtypeStruct((16, 48, lanes), F32),
        [pltpu.VMEM((GROUP, HALO + tokens, lanes), F32)],
        flops=62 * tokens * width * 100,
        moved=4 * tokens * width,
    )(ring, glu, halo, grad, gain_part)


def input_kernel(ring, grad, tail, taps, value, gate, grad_value, grad_gate, wide):
    end = ring[0] + ring[1] == 6
    tokens = grad.shape[0]
    lanes = wide.shape[2]
    for i in range(GROUP):
        at = slice(i * lanes, (i + 1) * lanes)
        wide[i, pl.ds(0, tokens), :] = grad[:, at].astype(F32)
        wide[i, pl.ds(tokens, HALO), :] = jnp.where(end, 0.0, tail[:, at].astype(F32))
        acc = jnp.zeros((tokens, lanes), F32)
        for j in range(31):
            acc = acc + taps[i, pl.ds(j, 1), :] * wide[i, pl.ds(30 - j, tokens), :]
        grad_glu = acc.astype(BF16).astype(F32)
        sig = jax.nn.sigmoid(gate[:, at].astype(F32))
        grad_value[:, at] = (grad_glu * sig).astype(BF16)
        grad_gate[:, at] = (grad_glu * value[:, at].astype(F32) * sig * (1.0 - sig)).astype(BF16)


def input_backward(ring, grad, tail, taps, value, gate):
    tokens, width = grad.shape
    lanes = width // 16
    column = lambda rows: pl.BlockSpec((rows, GROUP * lanes), lambda i, ring: (0, i))
    return call(
        input_kernel,
        (16 // GROUP,),
        [
            column(tokens),
            column(HALO),
            pl.BlockSpec((GROUP, 32, lanes), lambda i, ring: (i, 0, 0)),
            column(tokens),
            column(tokens),
        ],
        [column(tokens)] * 2,
        [jax.ShapeDtypeStruct((tokens, width), BF16)] * 2,
        [pltpu.VMEM((GROUP, HALO + tokens, lanes), F32)],
        flops=62 * tokens * width * 100,
        moved=10 * tokens * width,
    )(ring, grad, tail, taps, value, gate)


def from_everyone(shard, axis):
    count = lax.axis_size(axis)
    return lax.all_to_all(jnp.broadcast_to(shard[None], (count, *shard.shape)), axis, 0, 0, tiled=True)


EARLY = [
    (half, k, pair, 2 * half + out, at)
    for half in range(2)
    for k, pair, out, at in ((2, 0, 0, 0), (1, 1, 0, 2), (2, 1, 1, 0), (3, 0, 1, 2))
]
REST = [
    (half, k, pair, 3 * half + out, at)
    for half in range(2)
    for k, pair, out, at in ((1, 0, 0, 0), (3, 1, 1, 0), (0, 0, 2, 0), (0, 1, 2, 2))
]


def step(value_half, gate_half, upstream, conv_taps, norm_gain, out_weight):
    value, gate, upstream = value_half[0], gate_half[0], upstream[0]
    tokens, width = value.shape
    lanes = width // 16
    ring = jnp.stack([lax.axis_index(axis) for axis in (Y, X, Z, CORE)]).astype(jnp.int32)
    gain = norm_gain[None]

    weight = lax.all_gather(out_weight, DP, axis=0, tiled=True)
    tail = slice(tokens - HALO, tokens)
    glu_tail = (value[tail].astype(F32) * jax.nn.sigmoid(gate[tail].astype(F32))).astype(BF16)
    halo = lax.ppermute(glu_tail, SP, [(i, (i + 1) % 16) for i in range(16)])
    taps = from_everyone(jnp.pad(conv_taps, ((0, 1), (0, 0))), SP)

    turned, turned_away = turn(ring, upstream)
    turned_other = shift(turned_away, CORE, 1)

    glu, act, conv, mean, inv = forward(ring, value, gate, halo, taps, tie(gain, turned))
    act_other = shift(act, CORE, 1)
    early = outer(EARLY, ring, turned, turned_other, act, act_other)
    rest = outer(REST, ring, turned, turned_other, act, act_other)
    early, rest = (early[:2], early[2:]), (rest[:3], rest[3:])

    opened = [ring_open(axis, *part) for axis, part in zip((X, Y), early)]
    sums = [ring_sums(pair, *part[:2]) for pair, part in zip(opened, rest)]
    halves = [
        ring_close(axis, pair, late, part[2][:2], part[2][2:])
        for axis, pair, late, part in zip((X, Y), opened, sums, rest)
    ]
    grad, grad_head, gain_part = norm_backward(ring, upstream, weight, conv, mean, inv, tie(gain, sums))
    next_head = lax.ppermute(grad_head, SP, [((i + 1) % 16, i) for i in range(16)])

    pieces = [cut(*half) for half in halves]
    opened = [ring_open(axis, *piece[0]) for axis, piece in zip((Y, X), pieces)]
    sums = [ring_sums(pair, *piece[1]) for pair, piece in zip(opened, pieces)]
    closed = [ring_close(axis, pair, late, *piece[2]) for axis, pair, late, piece in zip((Y, X), opened, sums, pieces)]
    terms = taps_backward(ring, glu, halo, grad, gain_part)
    mine = lax.all_to_all(terms, SP, 0, 0, tiled=True)
    mine = jnp.sum(mine, axis=0)
    mine = mine + shift(mine, CORE, 1)

    scattered = jnp.concatenate([rows for half in closed for rows in half]).reshape(8, lanes, lanes)
    merged = jnp.concatenate([scattered, jnp.broadcast_to(mine[None], (8, *mine.shape))], axis=1).astype(BF16)
    merged = lax.all_to_all(merged, Z, 0, 0, tiled=True)
    merged = jnp.sum(merged.astype(F32), axis=0)
    grad_value, grad_gate = input_backward(ring, grad, next_head, taps, value, gate)

    owned, mine = merged[:lanes].astype(BF16), merged[lanes:]
    grad_weight = place(ring, plane_column(plane_row(owned)))
    grad_taps = mine[:31]
    grad_gain = mine[32:].reshape(width)
    return grad_value[None], grad_gate[None], grad_taps, grad_gain, grad_weight


def solution(mesh):
    torus = Mesh(mesh.devices.reshape(4, 4, 8, 2), (Y, X, Z, CORE))
    placed = (P(DP, SP, None), P(DP, SP, None), P(DP, SP, None), P(None, SP), P(), P(DP, None))
    return jax.shard_map(
        step,
        mesh=torus,
        in_specs=placed,
        out_specs=(P(DP, SP, None), P(DP, SP, None), P(None, SP), P(), P(DP, None)),
        check_vma=False,
    )
```

```python
import functools

import jax
import jax.numpy as jnp
from jax import lax
from jax.experimental import pallas as pl
from jax.experimental.pallas import tpu as pltpu
from jax.sharding import Mesh
from jax.sharding import PartitionSpec as P

DP = ("dp_0", "dp_1")
SP = ("sp_0", "sp_1")
Y, X, Z, CORE = "sp_0", "sp_1", "dp_0", "dp_1"
NORM_EPS = 1e-05
HALO = 32
GROUP = 4
VMEM_MIB = {'forward': 60, 'input_backward': 60, 'turn': 16, 'outer_early': 16, 'outer_rest': 16, 'place': 16, 'taps_backward': 16, 'norm_backward': 52}
INTERPRET = False
F32, BF16 = jnp.float32, jnp.bfloat16


def call(kernel, name, grid, in_specs, out_specs, out_shape, scratch, flops=0, moved=0):
    return pl.pallas_call(
        kernel,
        grid_spec=pltpu.PrefetchScalarGridSpec(
            num_scalar_prefetch=1,
            grid=grid,
            in_specs=in_specs,
            out_specs=out_specs,
            scratch_shapes=scratch,
        ),
        out_shape=out_shape,
        compiler_params=pltpu.CompilerParams(
            dimension_semantics=("arbitrary",) * len(grid), vmem_limit_bytes=VMEM_MIB.get(name, 48) * 1024 * 1024
        ),
        cost_estimate=pl.CostEstimate(flops=flops, bytes_accessed=moved, transcendentals=0),
        interpret=INTERPRET,
    )


def shift(value, axis, amount):
    count = lax.axis_size(axis)
    return lax.ppermute(value, axis, [(i, (i + amount) % count) for i in range(count)])


def forward_kernel(ring, value, gate, halo, taps, gain, glu, act, conv, mean, inv, wide, held, total):
    step = pl.program_id(0)
    start = ring[0] + ring[1] == 0
    tokens = value.shape[0]
    blocks, _, lanes = held.shape

    @pl.when(step == 0)
    def _():
        total[...] = jnp.zeros_like(total)

    for i in range(GROUP):
        at = slice(i * lanes, (i + 1) * lanes)
        block = step * GROUP + i
        gated = (value[:, at].astype(F32) * jax.nn.sigmoid(gate[:, at].astype(F32))).astype(BF16)
        glu[:, at] = gated
        wide[i, pl.ds(0, HALO), :] = jnp.where(start, 0.0, halo[:, at].astype(F32))
        wide[i, pl.ds(HALO, tokens), :] = gated.astype(F32)
        acc = jnp.zeros((tokens, lanes), F32)
        for j in range(31):
            acc = acc + taps[i, pl.ds(j, 1), :] * wide[i, pl.ds(2 + j, tokens), :]
        rounded = acc.astype(BF16)
        conv[:, pl.ds(pl.multiple_of(block * lanes, lanes), lanes)] = rounded
        rounded = rounded.astype(F32)
        held[block] = rounded
        total[...] += rounded

    @pl.when(step == pl.num_programs(0) - 1)
    def _():
        width = blocks * lanes
        mu = jnp.sum(total[...], axis=1, keepdims=True) / width
        mu = jnp.broadcast_to(mu, (tokens, lanes))
        mean[...] = mu

        def squares(i, acc):
            centered = held[i] - mean[...]
            return acc + centered * centered

        squared = lax.fori_loop(0, blocks, squares, jnp.zeros((tokens, lanes), F32))
        var = jnp.sum(squared, axis=1, keepdims=True) / width
        inv[...] = jnp.broadcast_to(lax.rsqrt(var + NORM_EPS), (tokens, lanes))

        def finish(i, carry):
            at = pl.ds(pl.multiple_of(i * lanes, lanes), lanes)
            scaled = (held[i] - mean[...]) * inv[...] * gain[:, at]
            act[:, at] = (scaled * jax.nn.sigmoid(scaled)).astype(BF16)
            return carry

        lax.fori_loop(0, blocks, finish, 0)


def forward(ring, value, gate, halo, taps, gain):
    tokens, width = value.shape
    lanes = width // 16
    column = lambda rows: pl.BlockSpec((rows, GROUP * lanes), lambda i, ring: (0, i))
    whole = lambda *shape: pl.BlockSpec(shape, lambda i, ring: (0,) * len(shape))
    return call(
        forward_kernel,
        "forward",
        (16 // GROUP,),
        [
            column(tokens),
            column(tokens),
            column(HALO),
            pl.BlockSpec((GROUP, 32, lanes), lambda i, ring: (i, 0, 0)),
            whole(1, width),
        ],
        [column(tokens), whole(tokens, width), whole(tokens, width), whole(tokens, lanes), whole(tokens, lanes)],
        [
            jax.ShapeDtypeStruct((tokens, width), BF16),
            jax.ShapeDtypeStruct((tokens, width), BF16),
            jax.ShapeDtypeStruct((tokens, width), BF16),
            jax.ShapeDtypeStruct((tokens, lanes), F32),
            jax.ShapeDtypeStruct((tokens, lanes), F32),
        ],
        [
            pltpu.VMEM((GROUP, HALO + tokens, lanes), F32),
            pltpu.VMEM((16, tokens, lanes), F32),
            pltpu.VMEM((tokens, lanes), F32),
        ],
        flops=62 * tokens * width * 100,
        moved=10 * tokens * width,
    )(ring, value, gate, halo, taps, gain)


def turn_kernel(ring, upstream, own, other):
    lanes = own.shape[1]
    core = ring[3]
    mine = upstream[:, pl.ds(pl.multiple_of(core * lanes, lanes), lanes)].astype(F32)
    own[0] = mine.T.astype(BF16)
    theirs = upstream[:, pl.ds(pl.multiple_of((1 - core) * lanes, lanes), lanes)].astype(F32)
    other[0] = theirs.T.astype(BF16)


def turn(ring, upstream):
    tokens, width = upstream.shape
    lanes = width // 16
    out = pl.BlockSpec((1, lanes, tokens), lambda i, ring: (i, 0, 0))
    shape = jax.ShapeDtypeStruct((8, lanes, tokens), BF16)
    return call(
        turn_kernel,
        "turn",
        (8,),
        [pl.BlockSpec((tokens, 2 * lanes), lambda i, ring: (0, i))],
        [out, out],
        [shape, shape],
        [],
        flops=tokens * width * 100,
        moved=4 * tokens * width,
    )(ring, upstream)


def outer_kernel(plan, ring, turned, turned_other, act, act_other, *outs):
    lanes = turned.shape[1]
    tokens = turned.shape[2]
    y, x = ring[0], ring[1]

    def columns(source, ky, kx):
        block = lax.rem(y + ky, 4) * 4 + lax.rem(x + kx, 4)
        return source[:, pl.ds(pl.multiple_of(block * lanes, lanes), lanes)]

    for half, k, pair, target, at in plan:
        out = outs[target]
        rows = pl.ds(4 * half, 4)
        left = turned[rows].reshape(4 * lanes, tokens)
        left_other = turned_other[rows].reshape(4 * lanes, tokens)
        spots = [(2 * pair + i, k) if half == 0 else (k, 2 * pair + i) for i in range(2)]
        right = jnp.concatenate([columns(act, *spot) for spot in spots], axis=1)
        right_other = jnp.concatenate([columns(act_other, *spot) for spot in spots], axis=1)
        product = jnp.dot(left, right, preferred_element_type=F32)
        product = product + jnp.dot(left_other, right_other, preferred_element_type=F32)
        out[at] = product[:, :lanes].astype(BF16)
        out[at + 1] = product[:, lanes:].astype(BF16)


def outer(name, plan, ring, turned, turned_other, act, act_other):
    tokens, width = act.shape
    lanes = width // 16
    whole = lambda *shape: pl.BlockSpec(shape, lambda i, ring: (0,) * len(shape))
    sizes = [max(at for *_, target, at in plan if target == out) + 2 for out in range(plan[-1][3] + 1)]
    return call(
        functools.partial(outer_kernel, plan),
        name,
        (1,),
        [whole(8, lanes, tokens)] * 2 + [whole(tokens, width)] * 2,
        [whole(size, 4 * lanes, lanes) for size in sizes],
        [jax.ShapeDtypeStruct((size, 4 * lanes, lanes), BF16) for size in sizes],
        [],
        flops=2 * 2 * tokens * 8 * lanes * lanes * len(plan),
        moved=8 * tokens * width,
    )(ring, turned, turned_other, act, act_other)


def add(*terms):
    return sum(term.astype(F32) for term in terms)


def tie(values, after):
    return lax.optimization_barrier((values, after))[0]


def ring_open(axis, on, back):
    return shift(on, axis, 1), shift(back, axis, -1)


def ring_sums(opened, next_low, previous_high):
    on, back = opened
    count = on.shape[0] // 2
    return add(next_low, on[:count]).astype(BF16), add(previous_high, back[:count]).astype(BF16)


def ring_close(axis, opened, sums, own_low, own_high):
    on, back = opened
    count = on.shape[0] // 2
    late_on = shift(sums[0], axis, 1)
    late_back = shift(sums[1], axis, -1)
    return add(own_low, late_on, back[count:]), add(own_high, on[count:], late_back)


def cut(low, high):
    rows = low.shape[1] // 2
    block = lambda k, h: (low, high)[k // 2][k % 2, h * rows : (h + 1) * rows]
    on = jnp.concatenate([block(2, 0), block(1, 1)]).astype(BF16)
    back = jnp.concatenate([block(2, 1), block(3, 0)]).astype(BF16)
    return (on, back), (block(1, 0), block(3, 1)), (block(0, 0), block(0, 1))


def place_kernel(ring, blocks, out):
    count, _, lanes = blocks.shape
    for i in range(count):
        block = lax.rem(ring[0] + i // 4, 4) * 4 + lax.rem(ring[1] + i % 4, 4)
        out[:, pl.ds(pl.multiple_of(block * lanes, lanes), lanes)] = blocks[i].astype(F32)


def place(ring, blocks):
    count, rows, lanes = blocks.shape
    whole = lambda *shape: pl.BlockSpec(shape, lambda i, ring: (0,) * len(shape))
    return call(
        place_kernel,
        "place",
        (1,),
        [whole(count, rows, lanes)],
        whole(rows, count * lanes),
        jax.ShapeDtypeStruct((rows, count * lanes), F32),
        [],
        flops=count * rows * lanes,
        moved=6 * count * rows * lanes,
    )(ring, blocks)


def plane_row(shard):
    return jnp.stack([shard] + [shift(shard, X, -k) for k in range(1, 4)])


def plane_column(row):
    return jnp.concatenate([row] + [shift(row, Y, -k) for k in range(1, 4)])


def norm_kernel(
    ring, upstream, weight, conv, mean, inv, gain, grad, grad_head, gain_part, held, first, second
):
    step = pl.program_id(0)
    steps = held.shape[0]
    _, lanes = mean.shape
    wide = 2 * lanes

    @pl.when(step == 0)
    def _():
        first[...] = jnp.zeros_like(first)
        second[...] = jnp.zeros_like(second)

    grad_act = jnp.dot(upstream[...], weight[...], preferred_element_type=F32)
    for i in range(2):
        at = slice(i * lanes, (i + 1) * lanes)
        columns = pl.ds(pl.multiple_of((2 * step + i) * lanes, lanes), lanes)
        normed = (conv[:, columns].astype(F32) - mean[...]) * inv[...]
        scaled = normed * gain[:, at]
        sig = jax.nn.sigmoid(scaled)
        grad_scaled = grad_act[:, at] * sig * (1.0 + scaled * (1.0 - sig))
        gain_part[pl.ds(2 * step + i, 1), :] = jnp.sum(grad_scaled * normed, axis=0, keepdims=True)
        g = grad_scaled * gain[:, at]
        held[step, :, at] = g
        first[...] += g
        second[...] += g * normed

    @pl.when(step == steps - 1)
    def _():
        width = steps * wide
        first[...] = jnp.broadcast_to(jnp.sum(first[...], axis=1, keepdims=True) / width, first.shape)
        second[...] = jnp.broadcast_to(jnp.sum(second[...], axis=1, keepdims=True) / width, second.shape)

        def finish(i, carry):
            for j in range(2):
                at = slice(j * lanes, (j + 1) * lanes)
                to = pl.ds(pl.multiple_of((2 * i + j) * lanes, lanes), lanes)
                normed = (conv[:, to].astype(F32) - mean[...]) * inv[...]
                value = (inv[...] * (held[i, :, at] - first[...] - normed * second[...])).astype(BF16)
                grad[:, to] = value
                grad_head[:, to] = value[:HALO]
            return carry

        lax.fori_loop(0, steps, finish, 0)


def norm_backward(ring, upstream, weight, conv, mean, inv, gain):
    tokens, width = upstream.shape
    lanes = width // 16
    wide = 2 * lanes
    column = lambda rows: pl.BlockSpec((rows, wide), lambda i, ring: (0, i))
    whole = lambda *shape: pl.BlockSpec(shape, lambda i, ring: (0,) * len(shape))
    return call(
        norm_kernel,
        "norm_backward",
        (8,),
        [
            whole(tokens, width),
            column(width),
            whole(tokens, width),
            whole(tokens, lanes),
            whole(tokens, lanes),
            column(1),
        ],
        [whole(tokens, width), whole(HALO, width), whole(16, lanes)],
        [
            jax.ShapeDtypeStruct((tokens, width), BF16),
            jax.ShapeDtypeStruct((HALO, width), BF16),
            jax.ShapeDtypeStruct((16, lanes), F32),
        ],
        [
            pltpu.VMEM((8, tokens, wide), F32),
            pltpu.VMEM((tokens, lanes), F32),
            pltpu.VMEM((tokens, lanes), F32),
        ],
        flops=2 * tokens * width * width,
        moved=2 * width * width + 6 * tokens * width,
    )(ring, upstream, weight, conv, mean, inv, gain)


def taps_kernel(ring, glu, halo, grad, gain_part, out, wide):
    start = ring[0] + ring[1] == 0
    tokens = glu.shape[0]
    lanes = wide.shape[2]
    for i in range(GROUP):
        at = slice(i * lanes, (i + 1) * lanes)
        wide[i, pl.ds(0, HALO), :] = jnp.where(start, 0.0, halo[:, at].astype(F32))
        wide[i, pl.ds(HALO, tokens), :] = glu[:, at].astype(F32)
        g = grad[:, at].astype(F32)
        for j in range(31):
            out[i, pl.ds(j, 1), :] = jnp.sum(g * wide[i, pl.ds(2 + j, tokens), :], axis=0, keepdims=True)
        out[i, pl.ds(31, 1), :] = jnp.zeros((1, lanes), F32)
        out[i, pl.ds(32, 16), :] = gain_part[...]


def taps_backward(ring, glu, halo, grad, gain_part):
    tokens, width = glu.shape
    lanes = width // 16
    column = lambda rows: pl.BlockSpec((rows, GROUP * lanes), lambda i, ring: (0, i))
    return call(
        taps_kernel,
        "taps_backward",
        (16 // GROUP,),
        [column(tokens), column(HALO), column(tokens), pl.BlockSpec((16, lanes), lambda i, ring: (0, 0))],
        pl.BlockSpec((GROUP, 48, lanes), lambda i, ring: (i, 0, 0)),
        jax.ShapeDtypeStruct((16, 48, lanes), F32),
        [pltpu.VMEM((GROUP, HALO + tokens, lanes), F32)],
        flops=62 * tokens * width * 100,
        moved=4 * tokens * width,
    )(ring, glu, halo, grad, gain_part)


def input_kernel(ring, grad, tail, taps, value, gate, grad_value, grad_gate, wide):
    end = ring[0] + ring[1] == 6
    tokens = grad.shape[0]
    lanes = wide.shape[2]
    for i in range(GROUP):
        at = slice(i * lanes, (i + 1) * lanes)
        wide[i, pl.ds(0, tokens), :] = grad[:, at].astype(F32)
        wide[i, pl.ds(tokens, HALO), :] = jnp.where(end, 0.0, tail[:, at].astype(F32))
        acc = jnp.zeros((tokens, lanes), F32)
        for j in range(31):
            acc = acc + taps[i, pl.ds(j, 1), :] * wide[i, pl.ds(30 - j, tokens), :]
        grad_glu = acc.astype(BF16).astype(F32)
        sig = jax.nn.sigmoid(gate[:, at].astype(F32))
        grad_value[:, at] = (grad_glu * sig).astype(BF16)
        grad_gate[:, at] = (grad_glu * value[:, at].astype(F32) * sig * (1.0 - sig)).astype(BF16)


def input_backward(ring, grad, tail, taps, value, gate):
    tokens, width = grad.shape
    lanes = width // 16
    column = lambda rows: pl.BlockSpec((rows, GROUP * lanes), lambda i, ring: (0, i))
    return call(
        input_kernel,
        "input_backward",
        (16 // GROUP,),
        [
            column(tokens),
            column(HALO),
            pl.BlockSpec((GROUP, 32, lanes), lambda i, ring: (i, 0, 0)),
            column(tokens),
            column(tokens),
        ],
        [column(tokens)] * 2,
        [jax.ShapeDtypeStruct((tokens, width), BF16)] * 2,
        [pltpu.VMEM((GROUP, HALO + tokens, lanes), F32)],
        flops=62 * tokens * width * 100,
        moved=10 * tokens * width,
    )(ring, grad, tail, taps, value, gate)


def from_everyone(shard, axis):
    count = lax.axis_size(axis)
    return lax.all_to_all(jnp.broadcast_to(shard[None], (count, *shard.shape)), axis, 0, 0, tiled=True)


EARLY = [
    (half, k, pair, 2 * half + out, at)
    for half in range(2)
    for k, pair, out, at in ((2, 0, 0, 0), (1, 1, 0, 2), (2, 1, 1, 0), (3, 0, 1, 2))
]
REST = [
    (half, k, pair, 3 * half + out, at)
    for half in range(2)
    for k, pair, out, at in ((1, 0, 0, 0), (3, 1, 1, 0), (0, 0, 2, 0), (0, 1, 2, 2))
]


def step(value_half, gate_half, upstream, conv_taps, norm_gain, out_weight):
    value, gate, upstream = value_half[0], gate_half[0], upstream[0]
    tokens, width = value.shape
    lanes = width // 16
    ring = jnp.stack([lax.axis_index(axis) for axis in (Y, X, Z, CORE)]).astype(jnp.int32)
    gain = norm_gain[None]

    weight = lax.all_gather(out_weight, DP, axis=0, tiled=True)
    tail = slice(tokens - HALO, tokens)
    glu_tail = (value[tail].astype(F32) * jax.nn.sigmoid(gate[tail].astype(F32))).astype(BF16)
    halo = lax.ppermute(glu_tail, SP, [(i, (i + 1) % 16) for i in range(16)])
    taps = from_everyone(jnp.pad(conv_taps, ((0, 1), (0, 0))), SP)

    glu, act, conv, mean, inv = forward(ring, value, gate, halo, taps, gain)
    act_other = shift(act, CORE, 1)
    turned, turned_away = turn(tie(ring, act), upstream)
    turned_other = shift(turned_away, CORE, 1)
    early = outer("outer_early", EARLY, ring, turned, turned_other, act, act_other)
    rest = outer("outer_rest", REST, ring, turned, turned_other, act, act_other)
    early, rest = (early[:2], early[2:]), (rest[:3], rest[3:])

    opened = [ring_open(axis, *part) for axis, part in zip((X, Y), early)]
    sums = [ring_sums(pair, *part[:2]) for pair, part in zip(opened, rest)]
    halves = [
        ring_close(axis, pair, late, part[2][:2], part[2][2:])
        for axis, pair, late, part in zip((X, Y), opened, sums, rest)
    ]
    grad, grad_head, gain_part = norm_backward(ring, upstream, weight, conv, mean, inv, tie(gain, sums))
    next_head = lax.ppermute(grad_head, SP, [((i + 1) % 16, i) for i in range(16)])

    pieces = [cut(*half) for half in halves]
    opened = [ring_open(axis, *piece[0]) for axis, piece in zip((Y, X), pieces)]
    sums = [ring_sums(pair, *piece[1]) for pair, piece in zip(opened, pieces)]
    closed = [ring_close(axis, pair, late, *piece[2]) for axis, pair, late, piece in zip((Y, X), opened, sums, pieces)]
    terms = taps_backward(ring, glu, halo, grad, gain_part)
    mine = lax.all_to_all(terms, SP, 0, 0, tiled=True)
    mine = jnp.sum(mine, axis=0)
    mine = mine + shift(mine, CORE, 1)

    scattered = jnp.concatenate([rows for half in closed for rows in half]).reshape(8, lanes, lanes)
    merged = jnp.concatenate([scattered, jnp.broadcast_to(mine[None], (8, *mine.shape))], axis=1).astype(BF16)
    merged = lax.all_to_all(merged, Z, 0, 0, tiled=True)
    merged = jnp.sum(merged.astype(F32), axis=0)
    grad_value, grad_gate = input_backward(ring, grad, next_head, taps, value, gate)

    owned, mine = merged[:lanes].astype(BF16), merged[lanes:]
    grad_weight = place(ring, plane_column(plane_row(owned)))
    grad_taps = mine[:31]
    grad_gain = mine[32:].reshape(width)
    return grad_value[None], grad_gate[None], grad_taps, grad_gain, grad_weight


def solution(mesh):
    torus = Mesh(mesh.devices.reshape(4, 4, 8, 2), (Y, X, Z, CORE))
    placed = (P(DP, SP, None), P(DP, SP, None), P(DP, SP, None), P(None, SP), P(), P(DP, None))
    return jax.shard_map(
        step,
        mesh=torus,
        in_specs=placed,
        out_specs=(P(DP, SP, None), P(DP, SP, None), P(None, SP), P(), P(DP, None)),
        check_vma=False,
    )
```

```python
import functools

import jax
import jax.numpy as jnp
from jax import lax
from jax.experimental import pallas as pl
from jax.experimental.pallas import tpu as pltpu
from jax.sharding import Mesh
from jax.sharding import PartitionSpec as P

DP = ("dp_0", "dp_1")
SP = ("sp_0", "sp_1")
Y, X, Z, CORE = "sp_0", "sp_1", "dp_0", "dp_1"
NORM_EPS = 1e-05
HALO = 32
GROUP = 4
VMEM_MIB = {'forward': 60, 'input_backward': 60, 'turn': 16, 'outer_early': 16, 'outer_rest': 16, 'place': 16, 'taps_backward': 16, 'norm_backward': 52}
INTERPRET = False
F32, BF16 = jnp.float32, jnp.bfloat16


def call(kernel, name, grid, in_specs, out_specs, out_shape, scratch, flops=0, moved=0):
    return pl.pallas_call(
        kernel,
        grid_spec=pltpu.PrefetchScalarGridSpec(
            num_scalar_prefetch=1,
            grid=grid,
            in_specs=in_specs,
            out_specs=out_specs,
            scratch_shapes=scratch,
        ),
        out_shape=out_shape,
        compiler_params=pltpu.CompilerParams(
            dimension_semantics=("arbitrary",) * len(grid), vmem_limit_bytes=VMEM_MIB.get(name, 48) * 1024 * 1024
        ),
        cost_estimate=pl.CostEstimate(flops=flops, bytes_accessed=moved, transcendentals=0),
        interpret=INTERPRET,
    )


def shift(value, axis, amount):
    count = lax.axis_size(axis)
    return lax.ppermute(value, axis, [(i, (i + amount) % count) for i in range(count)])


def forward_kernel(ring, value, gate, halo, taps, gain, glu, act, conv, mean, inv, wide, held, total):
    step = pl.program_id(0)
    start = ring[0] + ring[1] == 0
    tokens = value.shape[0]
    blocks, _, lanes = held.shape

    @pl.when(step == 0)
    def _():
        total[...] = jnp.zeros_like(total)

    for i in range(GROUP):
        at = slice(i * lanes, (i + 1) * lanes)
        block = step * GROUP + i
        gated = (value[:, at].astype(F32) * jax.nn.sigmoid(gate[:, at].astype(F32))).astype(BF16)
        glu[:, at] = gated
        wide[i, pl.ds(0, HALO), :] = jnp.where(start, 0.0, halo[:, at].astype(F32))
        wide[i, pl.ds(HALO, tokens), :] = gated.astype(F32)
        acc = jnp.zeros((tokens, lanes), F32)
        for j in range(31):
            acc = acc + taps[i, pl.ds(j, 1), :] * wide[i, pl.ds(2 + j, tokens), :]
        rounded = acc.astype(BF16)
        conv[:, pl.ds(pl.multiple_of(block * lanes, lanes), lanes)] = rounded
        rounded = rounded.astype(F32)
        held[block] = rounded
        total[...] += rounded

    @pl.when(step == pl.num_programs(0) - 1)
    def _():
        width = blocks * lanes
        mu = jnp.sum(total[...], axis=1, keepdims=True) / width
        mu = jnp.broadcast_to(mu, (tokens, lanes))
        mean[...] = mu

        def squares(i, acc):
            centered = held[i] - mean[...]
            return acc + centered * centered

        squared = lax.fori_loop(0, blocks, squares, jnp.zeros((tokens, lanes), F32))
        var = jnp.sum(squared, axis=1, keepdims=True) / width
        inv[...] = jnp.broadcast_to(lax.rsqrt(var + NORM_EPS), (tokens, lanes))

        def finish(i, carry):
            at = pl.ds(pl.multiple_of(i * lanes, lanes), lanes)
            scaled = (held[i] - mean[...]) * inv[...] * gain[:, at]
            act[:, at] = (scaled * jax.nn.sigmoid(scaled)).astype(BF16)
            return carry

        lax.fori_loop(0, blocks, finish, 0)


def forward(ring, value, gate, halo, taps, gain):
    tokens, width = value.shape
    lanes = width // 16
    column = lambda rows: pl.BlockSpec((rows, GROUP * lanes), lambda i, ring: (0, i))
    whole = lambda *shape: pl.BlockSpec(shape, lambda i, ring: (0,) * len(shape))
    return call(
        forward_kernel,
        "forward",
        (16 // GROUP,),
        [
            column(tokens),
            column(tokens),
            column(HALO),
            pl.BlockSpec((GROUP, 32, lanes), lambda i, ring: (i, 0, 0)),
            whole(1, width),
        ],
        [column(tokens), whole(tokens, width), whole(tokens, width), whole(tokens, lanes), whole(tokens, lanes)],
        [
            jax.ShapeDtypeStruct((tokens, width), BF16),
            jax.ShapeDtypeStruct((tokens, width), BF16),
            jax.ShapeDtypeStruct((tokens, width), BF16),
            jax.ShapeDtypeStruct((tokens, lanes), F32),
            jax.ShapeDtypeStruct((tokens, lanes), F32),
        ],
        [
            pltpu.VMEM((GROUP, HALO + tokens, lanes), F32),
            pltpu.VMEM((16, tokens, lanes), F32),
            pltpu.VMEM((tokens, lanes), F32),
        ],
        flops=62 * tokens * width * 100,
        moved=10 * tokens * width,
    )(ring, value, gate, halo, taps, gain)


def turn_kernel(ring, upstream, own, other):
    lanes = own.shape[1]
    core = ring[3]
    mine = upstream[:, pl.ds(pl.multiple_of(core * lanes, lanes), lanes)].astype(F32)
    own[0] = mine.T.astype(BF16)
    theirs = upstream[:, pl.ds(pl.multiple_of((1 - core) * lanes, lanes), lanes)].astype(F32)
    other[0] = theirs.T.astype(BF16)


def turn(ring, upstream):
    tokens, width = upstream.shape
    lanes = width // 16
    out = pl.BlockSpec((1, lanes, tokens), lambda i, ring: (i, 0, 0))
    shape = jax.ShapeDtypeStruct((8, lanes, tokens), BF16)
    return call(
        turn_kernel,
        "turn",
        (8,),
        [pl.BlockSpec((tokens, 2 * lanes), lambda i, ring: (0, i))],
        [out, out],
        [shape, shape],
        [],
        flops=tokens * width * 100,
        moved=4 * tokens * width,
    )(ring, upstream)


def outer_kernel(plan, ring, turned, turned_other, act, act_other, *outs):
    lanes = turned.shape[1]
    tokens = turned.shape[2]
    y, x = ring[0], ring[1]

    def columns(source, ky, kx):
        block = lax.rem(y + ky, 4) * 4 + lax.rem(x + kx, 4)
        return source[:, pl.ds(pl.multiple_of(block * lanes, lanes), lanes)]

    for half, k, pair, target, at in plan:
        out = outs[target]
        rows = pl.ds(4 * half, 4)
        left = turned[rows].reshape(4 * lanes, tokens)
        left_other = turned_other[rows].reshape(4 * lanes, tokens)
        spots = [(2 * pair + i, k) if half == 0 else (k, 2 * pair + i) for i in range(2)]
        right = jnp.concatenate([columns(act, *spot) for spot in spots], axis=1)
        right_other = jnp.concatenate([columns(act_other, *spot) for spot in spots], axis=1)
        product = jnp.dot(left, right, preferred_element_type=F32)
        product = product + jnp.dot(left_other, right_other, preferred_element_type=F32)
        out[at] = product[:, :lanes].astype(BF16)
        out[at + 1] = product[:, lanes:].astype(BF16)


def outer(name, plan, ring, turned, turned_other, act, act_other):
    tokens, width = act.shape
    lanes = width // 16
    whole = lambda *shape: pl.BlockSpec(shape, lambda i, ring: (0,) * len(shape))
    sizes = [max(at for *_, target, at in plan if target == out) + 2 for out in range(plan[-1][3] + 1)]
    return call(
        functools.partial(outer_kernel, plan),
        name,
        (1,),
        [whole(8, lanes, tokens)] * 2 + [whole(tokens, width)] * 2,
        [whole(size, 4 * lanes, lanes) for size in sizes],
        [jax.ShapeDtypeStruct((size, 4 * lanes, lanes), BF16) for size in sizes],
        [],
        flops=2 * 2 * tokens * 8 * lanes * lanes * len(plan),
        moved=8 * tokens * width,
    )(ring, turned, turned_other, act, act_other)


def add(*terms):
    return sum(term.astype(F32) for term in terms)


def tie(values, after):
    return lax.optimization_barrier((values, after))[0]


def ring_open(axis, on, back):
    return shift(on, axis, 1), shift(back, axis, -1)


def ring_sums(opened, next_low, previous_high):
    on, back = opened
    count = on.shape[0] // 2
    return add(next_low, on[:count]).astype(BF16), add(previous_high, back[:count]).astype(BF16)


def ring_close(axis, opened, sums, own_low, own_high):
    on, back = opened
    count = on.shape[0] // 2
    late_on = shift(sums[0], axis, 1)
    late_back = shift(sums[1], axis, -1)
    return add(own_low, late_on, back[count:]), add(own_high, on[count:], late_back)


def place_kernel(ring, blocks, out):
    count, _, lanes = blocks.shape
    for i in range(count):
        block = lax.rem(ring[0] + i // 4, 4) * 4 + lax.rem(ring[1] + i % 4, 4)
        out[:, pl.ds(pl.multiple_of(block * lanes, lanes), lanes)] = blocks[i].astype(F32)


def place(ring, blocks):
    count, rows, lanes = blocks.shape
    whole = lambda *shape: pl.BlockSpec(shape, lambda i, ring: (0,) * len(shape))
    return call(
        place_kernel,
        "place",
        (1,),
        [whole(count, rows, lanes)],
        whole(rows, count * lanes),
        jax.ShapeDtypeStruct((rows, count * lanes), F32),
        [],
        flops=count * rows * lanes,
        moved=6 * count * rows * lanes,
    )(ring, blocks)


def plane_row(shard):
    return jnp.stack([shard] + [shift(shard, X, -k) for k in range(1, 4)])


def plane_column(row):
    return jnp.concatenate([row] + [shift(row, Y, -k) for k in range(1, 4)])


def norm_kernel(
    ring, upstream, weight, conv, mean, inv, gain, grad, grad_head, gain_part, held, first, second
):
    step = pl.program_id(0)
    steps = held.shape[0]
    _, lanes = mean.shape
    wide = 2 * lanes

    @pl.when(step == 0)
    def _():
        first[...] = jnp.zeros_like(first)
        second[...] = jnp.zeros_like(second)

    grad_act = jnp.dot(upstream[...], weight[...], preferred_element_type=F32)
    for i in range(2):
        at = slice(i * lanes, (i + 1) * lanes)
        columns = pl.ds(pl.multiple_of((2 * step + i) * lanes, lanes), lanes)
        normed = (conv[:, columns].astype(F32) - mean[...]) * inv[...]
        scaled = normed * gain[:, at]
        sig = jax.nn.sigmoid(scaled)
        grad_scaled = grad_act[:, at] * sig * (1.0 + scaled * (1.0 - sig))
        gain_part[pl.ds(2 * step + i, 1), :] = jnp.sum(grad_scaled * normed, axis=0, keepdims=True)
        g = grad_scaled * gain[:, at]
        held[step, :, at] = g
        first[...] += g
        second[...] += g * normed

    @pl.when(step == steps - 1)
    def _():
        width = steps * wide
        first[...] = jnp.broadcast_to(jnp.sum(first[...], axis=1, keepdims=True) / width, first.shape)
        second[...] = jnp.broadcast_to(jnp.sum(second[...], axis=1, keepdims=True) / width, second.shape)

        def finish(i, carry):
            for j in range(2):
                at = slice(j * lanes, (j + 1) * lanes)
                to = pl.ds(pl.multiple_of((2 * i + j) * lanes, lanes), lanes)
                normed = (conv[:, to].astype(F32) - mean[...]) * inv[...]
                value = (inv[...] * (held[i, :, at] - first[...] - normed * second[...])).astype(BF16)
                grad[:, to] = value
                grad_head[:, to] = value[:HALO]
            return carry

        lax.fori_loop(0, steps, finish, 0)


def norm_backward(ring, upstream, weight, conv, mean, inv, gain):
    tokens, width = upstream.shape
    lanes = width // 16
    wide = 2 * lanes
    column = lambda rows: pl.BlockSpec((rows, wide), lambda i, ring: (0, i))
    whole = lambda *shape: pl.BlockSpec(shape, lambda i, ring: (0,) * len(shape))
    return call(
        norm_kernel,
        "norm_backward",
        (8,),
        [
            whole(tokens, width),
            column(width),
            whole(tokens, width),
            whole(tokens, lanes),
            whole(tokens, lanes),
            column(1),
        ],
        [whole(tokens, width), whole(HALO, width), whole(16, lanes)],
        [
            jax.ShapeDtypeStruct((tokens, width), BF16),
            jax.ShapeDtypeStruct((HALO, width), BF16),
            jax.ShapeDtypeStruct((16, lanes), F32),
        ],
        [
            pltpu.VMEM((8, tokens, wide), F32),
            pltpu.VMEM((tokens, lanes), F32),
            pltpu.VMEM((tokens, lanes), F32),
        ],
        flops=2 * tokens * width * width,
        moved=2 * width * width + 6 * tokens * width,
    )(ring, upstream, weight, conv, mean, inv, gain)


def taps_kernel(ring, glu, halo, grad, gain_part, out, wide):
    start = ring[0] + ring[1] == 0
    tokens = glu.shape[0]
    lanes = wide.shape[2]
    for i in range(GROUP):
        at = slice(i * lanes, (i + 1) * lanes)
        wide[i, pl.ds(0, HALO), :] = jnp.where(start, 0.0, halo[:, at].astype(F32))
        wide[i, pl.ds(HALO, tokens), :] = glu[:, at].astype(F32)
        g = grad[:, at].astype(F32)
        for j in range(31):
            out[i, pl.ds(j, 1), :] = jnp.sum(g * wide[i, pl.ds(2 + j, tokens), :], axis=0, keepdims=True)
        out[i, pl.ds(31, 1), :] = jnp.zeros((1, lanes), F32)
        out[i, pl.ds(32, 16), :] = gain_part[...]


def taps_backward(ring, glu, halo, grad, gain_part):
    tokens, width = glu.shape
    lanes = width // 16
    column = lambda rows: pl.BlockSpec((rows, GROUP * lanes), lambda i, ring: (0, i))
    return call(
        taps_kernel,
        "taps_backward",
        (16 // GROUP,),
        [column(tokens), column(HALO), column(tokens), pl.BlockSpec((16, lanes), lambda i, ring: (0, 0))],
        pl.BlockSpec((GROUP, 48, lanes), lambda i, ring: (i, 0, 0)),
        jax.ShapeDtypeStruct((16, 48, lanes), F32),
        [pltpu.VMEM((GROUP, HALO + tokens, lanes), F32)],
        flops=62 * tokens * width * 100,
        moved=4 * tokens * width,
    )(ring, glu, halo, grad, gain_part)


def input_kernel(ring, grad, tail, taps, value, gate, grad_value, grad_gate, wide):
    end = ring[0] + ring[1] == 6
    tokens = grad.shape[0]
    lanes = wide.shape[2]
    for i in range(GROUP):
        at = slice(i * lanes, (i + 1) * lanes)
        wide[i, pl.ds(0, tokens), :] = grad[:, at].astype(F32)
        wide[i, pl.ds(tokens, HALO), :] = jnp.where(end, 0.0, tail[:, at].astype(F32))
        acc = jnp.zeros((tokens, lanes), F32)
        for j in range(31):
            acc = acc + taps[i, pl.ds(j, 1), :] * wide[i, pl.ds(30 - j, tokens), :]
        grad_glu = acc.astype(BF16).astype(F32)
        sig = jax.nn.sigmoid(gate[:, at].astype(F32))
        grad_value[:, at] = (grad_glu * sig).astype(BF16)
        grad_gate[:, at] = (grad_glu * value[:, at].astype(F32) * sig * (1.0 - sig)).astype(BF16)


def input_backward(ring, grad, tail, taps, value, gate):
    tokens, width = grad.shape
    lanes = width // 16
    column = lambda rows: pl.BlockSpec((rows, GROUP * lanes), lambda i, ring: (0, i))
    return call(
        input_kernel,
        "input_backward",
        (16 // GROUP,),
        [
            column(tokens),
            column(HALO),
            pl.BlockSpec((GROUP, 32, lanes), lambda i, ring: (i, 0, 0)),
            column(tokens),
            column(tokens),
        ],
        [column(tokens)] * 2,
        [jax.ShapeDtypeStruct((tokens, width), BF16)] * 2,
        [pltpu.VMEM((GROUP, HALO + tokens, lanes), F32)],
        flops=62 * tokens * width * 100,
        moved=10 * tokens * width,
    )(ring, grad, tail, taps, value, gate)


def from_everyone(shard, axis):
    count = lax.axis_size(axis)
    return lax.all_to_all(jnp.broadcast_to(shard[None], (count, *shard.shape)), axis, 0, 0, tiled=True)


EARLY = [
    (half, k, pair, 2 * half + out, at)
    for half in range(2)
    for k, pair, out, at in ((2, 0, 0, 0), (1, 1, 0, 2), (2, 1, 1, 0), (3, 0, 1, 2))
]
REST = [
    (half, k, pair, 3 * half + out, at)
    for half in range(2)
    for k, pair, out, at in ((1, 0, 0, 0), (3, 1, 1, 0), (0, 0, 2, 0), (0, 1, 2, 2))
]


def step(value_half, gate_half, upstream, conv_taps, norm_gain, out_weight):
    value, gate, upstream = value_half[0], gate_half[0], upstream[0]
    tokens, width = value.shape
    lanes = width // 16
    ring = jnp.stack([lax.axis_index(axis) for axis in (Y, X, Z, CORE)]).astype(jnp.int32)
    gain = norm_gain[None]

    weight = lax.all_gather(out_weight, DP, axis=0, tiled=True)
    tail = slice(tokens - HALO, tokens)
    glu_tail = (value[tail].astype(F32) * jax.nn.sigmoid(gate[tail].astype(F32))).astype(BF16)
    halo = lax.ppermute(glu_tail, SP, [(i, (i + 1) % 16) for i in range(16)])
    taps = from_everyone(jnp.pad(conv_taps, ((0, 1), (0, 0))), SP)

    glu, act, conv, mean, inv = forward(ring, value, gate, halo, taps, gain)
    act_other = shift(act, CORE, 1)
    turned, turned_away = turn(tie(ring, act), upstream)
    turned_other = shift(turned_away, CORE, 1)
    early = outer("outer_early", EARLY, ring, turned, turned_other, act, act_other)
    rest = outer("outer_rest", REST, ring, turned, turned_other, act, act_other)
    early, rest = (early[:2], early[2:]), (rest[:3], rest[3:])

    opened = [ring_open(axis, *part) for axis, part in zip((X, Y), early)]
    sums = [ring_sums(pair, *part[:2]) for pair, part in zip(opened, rest)]
    halves = [
        ring_close(axis, pair, late, part[2][:2], part[2][2:])
        for axis, pair, late, part in zip((X, Y), opened, sums, rest)
    ]
    grad, grad_head, gain_part = norm_backward(ring, upstream, weight, conv, mean, inv, tie(gain, sums))
    next_head = lax.ppermute(grad_head, SP, [((i + 1) % 16, i) for i in range(16)])

    closed = []
    for axis, (low, high) in zip((Y, X), halves):
        sent = ((1, low[1]), (2, high[0]), (3, high[1]))
        closed.append(add(low[0], *[shift(block.astype(BF16), axis, k) for k, block in sent]))
    terms = taps_backward(ring, glu, halo, grad, gain_part)
    mine = lax.all_to_all(terms, SP, 0, 0, tiled=True)
    mine = jnp.sum(mine, axis=0)
    mine = mine + shift(mine, CORE, 1)

    scattered = jnp.concatenate(closed).reshape(8, lanes, lanes)
    merged = jnp.concatenate([scattered, jnp.broadcast_to(mine[None], (8, *mine.shape))], axis=1).astype(BF16)
    merged = lax.all_to_all(merged, Z, 0, 0, tiled=True)
    merged = jnp.sum(merged.astype(F32), axis=0)
    grad_value, grad_gate = input_backward(ring, grad, next_head, taps, value, gate)

    owned, mine = merged[:lanes].astype(BF16), merged[lanes:]
    grad_weight = place(ring, plane_column(plane_row(owned)))
    grad_taps = mine[:31]
    grad_gain = mine[32:].reshape(width)
    return grad_value[None], grad_gate[None], grad_taps, grad_gain, grad_weight


def solution(mesh):
    torus = Mesh(mesh.devices.reshape(4, 4, 8, 2), (Y, X, Z, CORE))
    placed = (P(DP, SP, None), P(DP, SP, None), P(DP, SP, None), P(None, SP), P(), P(DP, None))
    return jax.shard_map(
        step,
        mesh=torus,
        in_specs=placed,
        out_specs=(P(DP, SP, None), P(DP, SP, None), P(None, SP), P(), P(DP, None)),
        check_vma=False,
    )
```

```python
import functools

import jax
import jax.numpy as jnp
from jax import lax
from jax.experimental import pallas as pl
from jax.experimental.pallas import tpu as pltpu
from jax.sharding import Mesh
from jax.sharding import PartitionSpec as P

DP = ("dp_0", "dp_1")
SP = ("sp_0", "sp_1")
Y, X, Z, CORE = "sp_0", "sp_1", "dp_0", "dp_1"
NORM_EPS = 1e-05
HALO = 32
GROUP = 4
VMEM_MIB = {'forward': 60, 'input_backward': 60, 'turn': 16, 'outer_early': 16, 'outer_rest': 16, 'place': 16, 'taps_backward': 16, 'norm_backward': 52}
INTERPRET = False
F32, BF16 = jnp.float32, jnp.bfloat16


def call(kernel, name, grid, in_specs, out_specs, out_shape, scratch, flops=0, moved=0):
    return pl.pallas_call(
        kernel,
        grid_spec=pltpu.PrefetchScalarGridSpec(
            num_scalar_prefetch=1,
            grid=grid,
            in_specs=in_specs,
            out_specs=out_specs,
            scratch_shapes=scratch,
        ),
        out_shape=out_shape,
        compiler_params=pltpu.CompilerParams(
            dimension_semantics=("arbitrary",) * len(grid), vmem_limit_bytes=VMEM_MIB.get(name, 48) * 1024 * 1024
        ),
        cost_estimate=pl.CostEstimate(flops=flops, bytes_accessed=moved, transcendentals=0),
        interpret=INTERPRET,
    )


def shift(value, axis, amount):
    count = lax.axis_size(axis)
    return lax.ppermute(value, axis, [(i, (i + amount) % count) for i in range(count)])


def forward_kernel(ring, value, gate, halo, taps, gain, glu, act, conv, mean, inv, wide, held, total):
    step = pl.program_id(0)
    start = ring[0] + ring[1] == 0
    tokens = value.shape[0]
    blocks, _, lanes = held.shape

    @pl.when(step == 0)
    def _():
        total[...] = jnp.zeros_like(total)

    for i in range(GROUP):
        at = slice(i * lanes, (i + 1) * lanes)
        block = step * GROUP + i
        gated = (value[:, at].astype(F32) * jax.nn.sigmoid(gate[:, at].astype(F32))).astype(BF16)
        glu[:, at] = gated
        wide[i, pl.ds(0, HALO), :] = jnp.where(start, 0.0, halo[:, at].astype(F32))
        wide[i, pl.ds(HALO, tokens), :] = gated.astype(F32)
        acc = jnp.zeros((tokens, lanes), F32)
        for j in range(31):
            acc = acc + taps[i, pl.ds(j, 1), :] * wide[i, pl.ds(2 + j, tokens), :]
        rounded = acc.astype(BF16)
        conv[:, pl.ds(pl.multiple_of(block * lanes, lanes), lanes)] = rounded
        rounded = rounded.astype(F32)
        held[block] = rounded
        total[...] += rounded

    @pl.when(step == pl.num_programs(0) - 1)
    def _():
        width = blocks * lanes
        mu = jnp.sum(total[...], axis=1, keepdims=True) / width
        mu = jnp.broadcast_to(mu, (tokens, lanes))
        mean[...] = mu

        def squares(i, acc):
            centered = held[i] - mean[...]
            return acc + centered * centered

        squared = lax.fori_loop(0, blocks, squares, jnp.zeros((tokens, lanes), F32))
        var = jnp.sum(squared, axis=1, keepdims=True) / width
        inv[...] = jnp.broadcast_to(lax.rsqrt(var + NORM_EPS), (tokens, lanes))

        def finish(i, carry):
            at = pl.ds(pl.multiple_of(i * lanes, lanes), lanes)
            scaled = (held[i] - mean[...]) * inv[...] * gain[:, at]
            act[:, at] = (scaled * jax.nn.sigmoid(scaled)).astype(BF16)
            return carry

        lax.fori_loop(0, blocks, finish, 0)


def forward(ring, value, gate, halo, taps, gain):
    tokens, width = value.shape
    lanes = width // 16
    column = lambda rows: pl.BlockSpec((rows, GROUP * lanes), lambda i, ring: (0, i))
    whole = lambda *shape: pl.BlockSpec(shape, lambda i, ring: (0,) * len(shape))
    return call(
        forward_kernel,
        "forward",
        (16 // GROUP,),
        [
            column(tokens),
            column(tokens),
            column(HALO),
            pl.BlockSpec((GROUP, 32, lanes), lambda i, ring: (i, 0, 0)),
            whole(1, width),
        ],
        [column(tokens), whole(tokens, width), whole(tokens, width), whole(tokens, lanes), whole(tokens, lanes)],
        [
            jax.ShapeDtypeStruct((tokens, width), BF16),
            jax.ShapeDtypeStruct((tokens, width), BF16),
            jax.ShapeDtypeStruct((tokens, width), BF16),
            jax.ShapeDtypeStruct((tokens, lanes), F32),
            jax.ShapeDtypeStruct((tokens, lanes), F32),
        ],
        [
            pltpu.VMEM((GROUP, HALO + tokens, lanes), F32),
            pltpu.VMEM((16, tokens, lanes), F32),
            pltpu.VMEM((tokens, lanes), F32),
        ],
        flops=62 * tokens * width * 100,
        moved=10 * tokens * width,
    )(ring, value, gate, halo, taps, gain)


def turn_kernel(ring, upstream, own, other):
    lanes = own.shape[1]
    core = ring[3]
    mine = upstream[:, pl.ds(pl.multiple_of(core * lanes, lanes), lanes)].astype(F32)
    own[0] = mine.T.astype(BF16)
    theirs = upstream[:, pl.ds(pl.multiple_of((1 - core) * lanes, lanes), lanes)].astype(F32)
    other[0] = theirs.T.astype(BF16)


def turn(ring, upstream):
    tokens, width = upstream.shape
    lanes = width // 16
    out = pl.BlockSpec((1, lanes, tokens), lambda i, ring: (i, 0, 0))
    shape = jax.ShapeDtypeStruct((8, lanes, tokens), BF16)
    return call(
        turn_kernel,
        "turn",
        (8,),
        [pl.BlockSpec((tokens, 2 * lanes), lambda i, ring: (0, i))],
        [out, out],
        [shape, shape],
        [],
        flops=tokens * width * 100,
        moved=4 * tokens * width,
    )(ring, upstream)


def outer_kernel(plan, ring, turned, turned_other, act, act_other, *outs):
    lanes = turned.shape[1]
    tokens = turned.shape[2]
    y, x = ring[0], ring[1]

    def columns(source, ky, kx):
        block = lax.rem(y + ky, 4) * 4 + lax.rem(x + kx, 4)
        return source[:, pl.ds(pl.multiple_of(block * lanes, lanes), lanes)]

    for half, k, pair, target, at in plan:
        out = outs[target]
        rows = pl.ds(4 * half, 4)
        left = turned[rows].reshape(4 * lanes, tokens)
        left_other = turned_other[rows].reshape(4 * lanes, tokens)
        spots = [(2 * pair + i, k) if half == 0 else (k, 2 * pair + i) for i in range(2)]
        right = jnp.concatenate([columns(act, *spot) for spot in spots], axis=1)
        right_other = jnp.concatenate([columns(act_other, *spot) for spot in spots], axis=1)
        product = jnp.dot(left, right, preferred_element_type=F32)
        product = product + jnp.dot(left_other, right_other, preferred_element_type=F32)
        out[at] = product[:, :lanes].astype(BF16)
        out[at + 1] = product[:, lanes:].astype(BF16)


def outer(name, plan, ring, turned, turned_other, act, act_other):
    tokens, width = act.shape
    lanes = width // 16
    whole = lambda *shape: pl.BlockSpec(shape, lambda i, ring: (0,) * len(shape))
    sizes = [max(at for *_, target, at in plan if target == out) + 2 for out in range(plan[-1][3] + 1)]
    return call(
        functools.partial(outer_kernel, plan),
        name,
        (1,),
        [whole(8, lanes, tokens)] * 2 + [whole(tokens, width)] * 2,
        [whole(size, 4 * lanes, lanes) for size in sizes],
        [jax.ShapeDtypeStruct((size, 4 * lanes, lanes), BF16) for size in sizes],
        [],
        flops=2 * 2 * tokens * 8 * lanes * lanes * len(plan),
        moved=8 * tokens * width,
    )(ring, turned, turned_other, act, act_other)


def add(*terms):
    return sum(term.astype(F32) for term in terms)


def tie(values, after):
    return lax.optimization_barrier((values, after))[0]


def ring_open(axis, on, back):
    return shift(on, axis, 1), shift(back, axis, -1)


def ring_sums(opened, next_low, previous_high):
    on, back = opened
    count = on.shape[0] // 2
    return add(next_low, on[:count]).astype(BF16), add(previous_high, back[:count]).astype(BF16)


def ring_close(axis, opened, sums, own_low, own_high):
    on, back = opened
    count = on.shape[0] // 2
    late_on = shift(sums[0], axis, 1)
    late_back = shift(sums[1], axis, -1)
    return add(own_low, late_on, back[count:]), add(own_high, on[count:], late_back)


def place_kernel(ring, blocks, out):
    count, _, lanes = blocks.shape
    for i in range(count):
        block = lax.rem(ring[0] + i // 4, 4) * 4 + lax.rem(ring[1] + i % 4, 4)
        out[:, pl.ds(pl.multiple_of(block * lanes, lanes), lanes)] = blocks[i].astype(F32)


def place(ring, blocks):
    count, rows, lanes = blocks.shape
    whole = lambda *shape: pl.BlockSpec(shape, lambda i, ring: (0,) * len(shape))
    return call(
        place_kernel,
        "place",
        (1,),
        [whole(count, rows, lanes)],
        whole(rows, count * lanes),
        jax.ShapeDtypeStruct((rows, count * lanes), F32),
        [],
        flops=count * rows * lanes,
        moved=6 * count * rows * lanes,
    )(ring, blocks)


def around(value, axis):
    across = shift(value, axis, -2)
    return [value, shift(value, axis, -1), across, shift(value, axis, -3)]


def plane_row(shard):
    return jnp.stack(around(shard, X))


def plane_column(row):
    return jnp.concatenate(around(row, Y))


def norm_kernel(
    ring, upstream, weight, conv, mean, inv, gain, grad, grad_head, gain_part, held, first, second
):
    step = pl.program_id(0)
    steps = held.shape[0]
    _, lanes = mean.shape
    wide = 2 * lanes

    @pl.when(step == 0)
    def _():
        first[...] = jnp.zeros_like(first)
        second[...] = jnp.zeros_like(second)

    grad_act = jnp.dot(upstream[...], weight[...], preferred_element_type=F32)
    for i in range(2):
        at = slice(i * lanes, (i + 1) * lanes)
        columns = pl.ds(pl.multiple_of((2 * step + i) * lanes, lanes), lanes)
        normed = (conv[:, columns].astype(F32) - mean[...]) * inv[...]
        scaled = normed * gain[:, at]
        sig = jax.nn.sigmoid(scaled)
        grad_scaled = grad_act[:, at] * sig * (1.0 + scaled * (1.0 - sig))
        gain_part[pl.ds(2 * step + i, 1), :] = jnp.sum(grad_scaled * normed, axis=0, keepdims=True)
        g = grad_scaled * gain[:, at]
        held[step, :, at] = g
        first[...] += g
        second[...] += g * normed

    @pl.when(step == steps - 1)
    def _():
        width = steps * wide
        first[...] = jnp.broadcast_to(jnp.sum(first[...], axis=1, keepdims=True) / width, first.shape)
        second[...] = jnp.broadcast_to(jnp.sum(second[...], axis=1, keepdims=True) / width, second.shape)

        def finish(i, carry):
            for j in range(2):
                at = slice(j * lanes, (j + 1) * lanes)
                to = pl.ds(pl.multiple_of((2 * i + j) * lanes, lanes), lanes)
                normed = (conv[:, to].astype(F32) - mean[...]) * inv[...]
                value = (inv[...] * (held[i, :, at] - first[...] - normed * second[...])).astype(BF16)
                grad[:, to] = value
                grad_head[:, to] = value[:HALO]
            return carry

        lax.fori_loop(0, steps, finish, 0)


def norm_backward(ring, upstream, weight, conv, mean, inv, gain):
    tokens, width = upstream.shape
    lanes = width // 16
    wide = 2 * lanes
    column = lambda rows: pl.BlockSpec((rows, wide), lambda i, ring: (0, i))
    whole = lambda *shape: pl.BlockSpec(shape, lambda i, ring: (0,) * len(shape))
    return call(
        norm_kernel,
        "norm_backward",
        (8,),
        [
            whole(tokens, width),
            column(width),
            whole(tokens, width),
            whole(tokens, lanes),
            whole(tokens, lanes),
            column(1),
        ],
        [whole(tokens, width), whole(HALO, width), whole(16, lanes)],
        [
            jax.ShapeDtypeStruct((tokens, width), BF16),
            jax.ShapeDtypeStruct((HALO, width), BF16),
            jax.ShapeDtypeStruct((16, lanes), F32),
        ],
        [
            pltpu.VMEM((8, tokens, wide), F32),
            pltpu.VMEM((tokens, lanes), F32),
            pltpu.VMEM((tokens, lanes), F32),
        ],
        flops=2 * tokens * width * width,
        moved=2 * width * width + 6 * tokens * width,
    )(ring, upstream, weight, conv, mean, inv, gain)


def taps_kernel(ring, glu, halo, grad, gain_part, out, wide):
    start = ring[0] + ring[1] == 0
    tokens = glu.shape[0]
    lanes = wide.shape[2]
    for i in range(GROUP):
        at = slice(i * lanes, (i + 1) * lanes)
        wide[i, pl.ds(0, HALO), :] = jnp.where(start, 0.0, halo[:, at].astype(F32))
        wide[i, pl.ds(HALO, tokens), :] = glu[:, at].astype(F32)
        g = grad[:, at].astype(F32)
        for j in range(31):
            out[i, pl.ds(j, 1), :] = jnp.sum(g * wide[i, pl.ds(2 + j, tokens), :], axis=0, keepdims=True)
        out[i, pl.ds(31, 1), :] = jnp.zeros((1, lanes), F32)
        out[i, pl.ds(32, 16), :] = gain_part[...]


def taps_backward(ring, glu, halo, grad, gain_part):
    tokens, width = glu.shape
    lanes = width // 16
    column = lambda rows: pl.BlockSpec((rows, GROUP * lanes), lambda i, ring: (0, i))
    return call(
        taps_kernel,
        "taps_backward",
        (16 // GROUP,),
        [column(tokens), column(HALO), column(tokens), pl.BlockSpec((16, lanes), lambda i, ring: (0, 0))],
        pl.BlockSpec((GROUP, 48, lanes), lambda i, ring: (i, 0, 0)),
        jax.ShapeDtypeStruct((16, 48, lanes), F32),
        [pltpu.VMEM((GROUP, HALO + tokens, lanes), F32)],
        flops=62 * tokens * width * 100,
        moved=4 * tokens * width,
    )(ring, glu, halo, grad, gain_part)


def input_kernel(ring, grad, tail, taps, value, gate, grad_value, grad_gate, wide):
    end = ring[0] + ring[1] == 6
    tokens = grad.shape[0]
    lanes = wide.shape[2]
    for i in range(GROUP):
        at = slice(i * lanes, (i + 1) * lanes)
        wide[i, pl.ds(0, tokens), :] = grad[:, at].astype(F32)
        wide[i, pl.ds(tokens, HALO), :] = jnp.where(end, 0.0, tail[:, at].astype(F32))
        acc = jnp.zeros((tokens, lanes), F32)
        for j in range(31):
            acc = acc + taps[i, pl.ds(j, 1), :] * wide[i, pl.ds(30 - j, tokens), :]
        grad_glu = acc.astype(BF16).astype(F32)
        sig = jax.nn.sigmoid(gate[:, at].astype(F32))
        grad_value[:, at] = (grad_glu * sig).astype(BF16)
        grad_gate[:, at] = (grad_glu * value[:, at].astype(F32) * sig * (1.0 - sig)).astype(BF16)


def input_backward(ring, grad, tail, taps, value, gate):
    tokens, width = grad.shape
    lanes = width // 16
    column = lambda rows: pl.BlockSpec((rows, GROUP * lanes), lambda i, ring: (0, i))
    return call(
        input_kernel,
        "input_backward",
        (16 // GROUP,),
        [
            column(tokens),
            column(HALO),
            pl.BlockSpec((GROUP, 32, lanes), lambda i, ring: (i, 0, 0)),
            column(tokens),
            column(tokens),
        ],
        [column(tokens)] * 2,
        [jax.ShapeDtypeStruct((tokens, width), BF16)] * 2,
        [pltpu.VMEM((GROUP, HALO + tokens, lanes), F32)],
        flops=62 * tokens * width * 100,
        moved=10 * tokens * width,
    )(ring, grad, tail, taps, value, gate)


def from_everyone(shard, axis):
    count = lax.axis_size(axis)
    return lax.all_to_all(jnp.broadcast_to(shard[None], (count, *shard.shape)), axis, 0, 0, tiled=True)


EARLY = [
    (half, k, pair, 2 * half + out, at)
    for half in range(2)
    for k, pair, out, at in ((2, 0, 0, 0), (1, 1, 0, 2), (2, 1, 1, 0), (3, 0, 1, 2))
]
REST = [
    (half, k, pair, 3 * half + out, at)
    for half in range(2)
    for k, pair, out, at in ((1, 0, 0, 0), (3, 1, 1, 0), (0, 0, 2, 0), (0, 1, 2, 2))
]


def step(value_half, gate_half, upstream, conv_taps, norm_gain, out_weight):
    value, gate, upstream = value_half[0], gate_half[0], upstream[0]
    tokens, width = value.shape
    lanes = width // 16
    ring = jnp.stack([lax.axis_index(axis) for axis in (Y, X, Z, CORE)]).astype(jnp.int32)
    gain = norm_gain[None]

    weight = lax.all_gather(out_weight, DP, axis=0, tiled=True)
    tail = slice(tokens - HALO, tokens)
    glu_tail = (value[tail].astype(F32) * jax.nn.sigmoid(gate[tail].astype(F32))).astype(BF16)
    halo = lax.ppermute(glu_tail, SP, [(i, (i + 1) % 16) for i in range(16)])
    taps = from_everyone(jnp.pad(conv_taps, ((0, 1), (0, 0))), SP)

    glu, act, conv, mean, inv = forward(ring, value, gate, halo, taps, gain)
    act_other = shift(act, CORE, 1)
    turned, turned_away = turn(tie(ring, act), upstream)
    turned_other = shift(turned_away, CORE, 1)
    early = outer("outer_early", EARLY, ring, turned, turned_other, act, act_other)
    rest = outer("outer_rest", REST, ring, turned, turned_other, act, act_other)
    early, rest = (early[:2], early[2:]), (rest[:3], rest[3:])

    opened = [ring_open(axis, *part) for axis, part in zip((X, Y), early)]
    sums = [ring_sums(pair, *part[:2]) for pair, part in zip(opened, rest)]
    halves = [
        ring_close(axis, pair, late, part[2][:2], part[2][2:])
        for axis, pair, late, part in zip((X, Y), opened, sums, rest)
    ]
    grad, grad_head, gain_part = norm_backward(ring, upstream, weight, conv, mean, inv, tie(gain, sums))
    next_head = lax.ppermute(grad_head, SP, [((i + 1) % 16, i) for i in range(16)])

    terms = taps_backward(ring, glu, halo, grad, gain_part)
    mine = lax.all_to_all(terms, SP, 0, 0, tiled=True)
    mine = jnp.sum(mine, axis=0)
    mine = mine + shift(mine, CORE, 1)

    closed = []
    for axis, (low, high) in zip((Y, X), halves):
        sent = ((1, low[1]), (2, high[0]), (3, high[1]))
        got = tie([shift(block.astype(BF16), axis, k) for k, block in sent], mine)
        closed.append(add(low[0], *got))

    scattered = jnp.concatenate(closed).reshape(8, lanes, lanes)
    merged = jnp.concatenate([scattered, jnp.broadcast_to(mine[None], (8, *mine.shape))], axis=1).astype(BF16)
    merged = lax.all_to_all(merged, Z, 0, 0, tiled=True)
    merged = jnp.sum(merged.astype(F32), axis=0)
    grad_value, grad_gate = input_backward(ring, grad, next_head, taps, value, gate)

    owned, mine = merged[:lanes].astype(BF16), merged[lanes:]
    grad_weight = place(ring, plane_column(plane_row(owned)))
    grad_taps = mine[:31]
    grad_gain = mine[32:].reshape(width)
    return grad_value[None], grad_gate[None], grad_taps, grad_gain, grad_weight


def solution(mesh):
    torus = Mesh(mesh.devices.reshape(4, 4, 8, 2), (Y, X, Z, CORE))
    placed = (P(DP, SP, None), P(DP, SP, None), P(DP, SP, None), P(None, SP), P(), P(DP, None))
    return jax.shard_map(
        step,
        mesh=torus,
        in_specs=placed,
        out_specs=(P(DP, SP, None), P(DP, SP, None), P(None, SP), P(), P(DP, None)),
        check_vma=False,
    )
```
